32 devices in a mesh: ep: 8 (over z, y), tp: 4 (over x, core).
Axes of the slice: x: 2, y: 2, z: 4, core: 2. Of those that a mesh axis runs over, the one named last changes fastest.
Arguments:
- tokens: bfloat16 [256, 2048], P('ep'), may hold values from -6 to 6
- gain_mix: bfloat16 [2048], replicated, may hold values from 0.099609375 to 1.8984375
- gain_ffn: bfloat16 [2048], replicated, may hold values from 0.099609375 to 1.8984375
- w_query: bfloat16 [2048, 1024], P('ep', 'tp'), may hold values from -0.125 to 0.125
- w_key: bfloat16 [2048, 1024], P('ep', 'tp'), may hold values from -0.125 to 0.125
- w_value: bfloat16 [2048, 1024], P('ep', 'tp'), may hold values from -0.125 to 0.125
- w_outgate: bfloat16 [2048, 1024], P('ep', 'tp'), may hold values from -0.125 to 0.125
- w_ingate: bfloat16 [2048, 8], replicated, may hold values from -0.125 to 0.125
- w_forget: bfloat16 [2048, 8], replicated, may hold values from -0.125 to 0.125
- bias_in: float32 [8], replicated, may hold values from -2 to 2
- bias_forget: float32 [8], replicated, may hold values from -1 to 3
- w_proj: bfloat16 [1024, 2048], P('tp'), may hold values from -0.1875 to 0.1875
- matrix_state: float32 [256, 8, 128, 128], P('ep', 'tp'), may hold values from -0.6 to 0.6
- normal_state: float32 [256, 8, 128], P('ep', 'tp'), may hold values from -0.6 to 0.6
- stab_state: float32 [256, 8], P('ep', 'tp'), may hold values from -1 to 1
- route_ids: int32 [256, 2], P('ep'), may hold values from 0 to 3, all different within a row; in each aligned block of 32 rows (0 to 31, 32 to 63, ...) at most 32 rows name the same one
- route_weights: float32 [256, 2], P('ep'), may hold values from 0.1 to 1
- w_exp_gate: bfloat16 [8, 2048, 1536], P('ep', None, 'tp'), may hold values from -0.125 to 0.125
- w_exp_up: bfloat16 [8, 2048, 1536], P('ep', None, 'tp'), may hold values from -0.125 to 0.125
- w_exp_down: bfloat16 [8, 1536, 2048], P('ep', 'tp'), may hold values from -0.109375 to 0.109375
Outputs:
- mixed_out: bfloat16 [256, 2048], P('ep', 'tp')
- matrix_out: float32 [256, 8, 128, 128], P('ep', 'tp')
- normal_out: float32 [256, 8, 128], P('ep', 'tp')
- stab_out: float32 [256, 8], P('ep', 'tp')
The draws below stay inside these ranges and needn't reach their ends.
Inputs may be any that keep to these rules, and one draw needn't show every extreme that they name: `route_ids`: each row names 2 different experts; among the rows of one index of ep no expert is named by more than 32 rows, and in every draw some expert is named by exactly 32 of them.
All inputs are finite; a program needn't handle non-finite values.
Results may differ from the reference program's by a relative error of at most 0.015.
Values may be sent and summed in bfloat16 or wider, within the bound.
No kernel may reach another device: no remote copies, remote signals or barrier semaphores. Data moves between devices by JAX's collectives and lax.ppermute only.
A program may use at most 64 MiB of HBM per device.

```python
import math
import jax
import jax.numpy as jnp
import numpy as np
from jax import lax

D = 2048
HEADS = 8
HEAD_DIM = 128
FF = 3072
TOPK = 2
SEQ_DEV = 32
WIDTH = 1024
SEQS = 256
EXPERTS = 4
CAP = 32
N_EP = 8
N_TP = 4


def shard_levels(stream_key, extent, split, low, largest):
    level = 1.0
    for dim, shards_of in split:
        draws = jax.random.uniform(jax.random.fold_in(jax.random.fold_in(stream_key, 6), dim), (shards_of,), jnp.float32, low / len(split), largest / len(split))
        level = level * jnp.repeat(jnp.exp(draws), extent[dim] // shards_of).reshape((-1,) + (1,) * (len(extent) - 1 - dim))
    return level


def shared_out(own_key, own, number, rows, count, top, most, lean):
    order = jax.random.permutation(own_key, count)
    heavy_load, common = portions_of(count, rows * top, most, lean, True), portions_of(count, rows * top, most, lean, False)
    places = jnp.arange(count)

    def named(tallies, turn):
        used = int((tallies > 0).sum())
        fixed = max(1, used // 4)
        moved = fixed + (places - fixed + turn * (used - fixed)) % max(1, count - fixed)
        return jnp.zeros((count,), jnp.int32).at[order[jnp.where(places < fixed, places, moved)]].set(jnp.asarray(tallies, jnp.int32))

    tallies = jnp.where(number % 4 == 0, named(heavy_load, number // 4), named(common, number - number // 4 - 1))
    mixed = jax.random.permutation(jax.random.fold_in(own, 3), count)
    donor, sink = mixed[0:count // 2 * 2:2], mixed[1:count // 2 * 2:2]
    room = jnp.minimum(tallies[donor] - 1, most - tallies[sink]) // 2
    room = jnp.where((donor == order[0]) | (sink == order[0]) | (tallies[sink] == 0), 0, jnp.maximum(room, 0))
    moved = jax.random.randint(jax.random.fold_in(own, 4), (count // 2,), 0, 1 << 20) % (room + 1)
    tallies = tallies.at[donor].add(-moved).at[sink].add(moved)
    items = jnp.searchsorted(jnp.cumsum(tallies), jnp.arange(rows * top), side="right").astype(jnp.int32)
    table = items.reshape(top, rows).T
    table = table[jax.random.permutation(jax.random.fold_in(own, 1), rows)]
    turn = jax.random.randint(jax.random.fold_in(own, 2), (rows, 1), 0, top)
    return jnp.take_along_axis(table, (jnp.arange(top)[None, :] + turn) % top, axis=1)


def portions_of(number_of, total, most, lean, full):
    portions = [(1 << 20) // math.isqrt(grade ** lean) + 1 for grade in range(1, number_of + 1)]
    largest = most if full else min(most, max(-(-total // number_of), total * portions[0] // sum(portions)))
    least = 1 if total - largest >= number_of - 1 else 0
    holding, surplus = [largest] + [least] * (number_of - 1), total - largest - least * (number_of - 1)
    while surplus > 0:
        movable = [i for i in range(1, number_of) if holding[i] < largest] or [i for i in range(1, number_of) if holding[i] < most]
        mass, budget = sum([portions[i] for i in movable]), surplus
        for i in movable:
            extra = min(most - holding[i], max(1, budget * portions[i] // mass), surplus)
            holding[i] = holding[i] + extra
            surplus = surplus - extra
    return np.array(holding)


def scatter_about(stream_key, dims, width, reach, split=(), held_as=jnp.bfloat16):
    level = shard_levels(stream_key, dims, split, -0.22, 0.18) if split else 1.0
    values = jax.random.normal(stream_key, dims, jnp.float32) * width * level
    return jnp.minimum(jnp.maximum(values, -reach), reach).astype(held_as)


def setup_inputs(seed: int = 0) -> dict:
    splits = jax.random.split(jax.random.key(seed), 21)
    tokens = scatter_about(splits[0], (SEQS, D), 1.0, 6.0, ((0, 8),))
    gain_mix = jnp.clip(1.0 + 0.18 * jax.random.normal(splits[1], (D,), jnp.float32), 0.099609375, 1.8984375).astype(jnp.bfloat16)
    gain_ffn = jnp.clip(1.0 + 0.18 * jax.random.normal(splits[2], (D,), jnp.float32), 0.099609375, 1.8984375).astype(jnp.bfloat16)
    w_query = scatter_about(splits[3], (D, WIDTH), D ** -0.5, 0.125, ((0, 8), (1, 4)))
    w_key = scatter_about(splits[4], (D, WIDTH), D ** -0.5, 0.125, ((0, 8), (1, 4)))
    w_value = scatter_about(splits[5], (D, WIDTH), D ** -0.5, 0.125, ((0, 8), (1, 4)))
    w_outgate = scatter_about(splits[6], (D, WIDTH), D ** -0.5, 0.125, ((0, 8), (1, 4)))
    w_ingate = scatter_about(splits[7], (D, HEADS), D ** -0.5, 0.125)
    w_forget = scatter_about(splits[8], (D, HEADS), D ** -0.5, 0.125)
    bias_in = jnp.clip(jax.random.uniform(splits[9], (HEADS,), jnp.float32, -2.0, 2.0), -2.0, 2.0)
    bias_forget = jnp.clip(jax.random.uniform(splits[10], (HEADS,), jnp.float32, -1.0, 3.0), -1.0, 3.0)
    w_proj = scatter_about(splits[11], (WIDTH, D), WIDTH ** -0.5, 0.1875, ((0, 4),))
    matrix_state = scatter_about(splits[12], (SEQS, HEADS, HEAD_DIM, HEAD_DIM), 0.1, 0.6, ((0, 8), (1, 4)), jnp.float32)
    normal_state = scatter_about(splits[13], (SEQS, HEADS, HEAD_DIM), 0.1, 0.6, ((0, 8), (1, 4)), jnp.float32)
    stab_state = jnp.clip(jax.random.uniform(splits[14], (SEQS, HEADS), jnp.float32, -1.0, 1.0) * shard_levels(splits[14], (SEQS, HEADS), ((0, 8), (1, 4)), -0.4, 0.0), -1.0, 1.0)
    route_ids_keys = jax.random.split(jax.random.fold_in(splits[15], 1), SEQS // SEQ_DEV)
    route_ids_turns = jax.random.permutation(jax.random.fold_in(splits[15], 3), SEQS // SEQ_DEV)
    route_ids = jax.vmap(lambda own, number: shared_out(jax.random.fold_in(splits[15], 2), own, number, SEQ_DEV, EXPERTS, TOPK, CAP, 1))(route_ids_keys, route_ids_turns).reshape((SEQS, TOPK))
    route_weights = jnp.clip(0.1 + 0.9 * jax.random.uniform(splits[16], (SEQS, TOPK), jnp.float32) ** shard_levels(splits[16], (SEQS, TOPK), ((0, 8),), -0.2, 0.2), 0.1, 1.0)
    w_exp_gate = scatter_about(splits[17], (2 * EXPERTS, D, FF // 2), D ** -0.5, 0.125, ((0, 8), (2, 4)))
    w_exp_up = scatter_about(splits[18], (2 * EXPERTS, D, FF // 2), D ** -0.5, 0.125, ((0, 8), (2, 4)))
    w_exp_down = scatter_about(splits[19], (2 * EXPERTS, FF // 2, D), FF ** -0.5, 0.109375, ((0, 8), (1, 4)))
    return {"tokens": tokens, "gain_mix": gain_mix, "gain_ffn": gain_ffn, "w_query": w_query, "w_key": w_key, "w_value": w_value, "w_outgate": w_outgate, "w_ingate": w_ingate, "w_forget": w_forget, "bias_in": bias_in, "bias_forget": bias_forget, "w_proj": w_proj, "matrix_state": matrix_state, "normal_state": normal_state, "stab_state": stab_state, "route_ids": route_ids, "route_weights": route_weights, "w_exp_gate": w_exp_gate, "w_exp_up": w_exp_up, "w_exp_down": w_exp_down}


norm_epsilon = 1e-06

def rms_scale(row_block, gain):
    wide = row_block.astype(jnp.float32)
    factor = lax.rsqrt(lax.optimization_barrier(jnp.mean(wide * wide, axis=-1, keepdims=True)) + norm_epsilon)
    return (wide * factor * gain.astype(jnp.float32)).astype(jnp.bfloat16)

def memory_step(query, key_rows, value_rows, gate_rows, in_pre, forget_pre, matrix_state, normal_state, stab_state):
    log_forget = jax.nn.log_sigmoid(forget_pre)
    stab_new = jnp.maximum(log_forget + stab_state, in_pre)
    carry = jnp.exp(log_forget + stab_state - stab_new)
    inflow = jnp.exp(in_pre - stab_new)
    scaled_keys = key_rows.astype(jnp.float32) * query.shape[-1] ** (-0.5)
    value_wide = value_rows.astype(jnp.float32)
    matrix_new = carry[..., None, None] * matrix_state + inflow[..., None, None] * scaled_keys[..., :, None] * value_wide[..., None, :]
    normal_new = carry[..., None] * normal_state + inflow[..., None] * scaled_keys
    query_wide = query.astype(jnp.float32)
    numer = jnp.einsum('shd,shde->she', query_wide, matrix_new, precision=lax.Precision.HIGHEST)
    denom = jnp.maximum(jnp.abs(lax.optimization_barrier(jnp.sum(query_wide * normal_new, axis=-1))), 1.0)
    hidden = numer / denom[..., None] * jax.nn.sigmoid(gate_rows.astype(jnp.float32))
    return (hidden, matrix_new, normal_new, stab_new)

def reference(tokens, gain_mix, gain_ffn, w_query, w_key, w_value, w_outgate, w_ingate, w_forget, bias_in, bias_forget, w_proj, matrix_state, normal_state, stab_state, route_ids, route_weights, w_exp_gate, w_exp_up, w_exp_down):
    normed = rms_scale(tokens, gain_mix)

    def project(weight):
        return jnp.dot(normed, weight, preferred_element_type=jnp.float32).astype(jnp.bfloat16).reshape(SEQS, HEADS, HEAD_DIM)
    query = project(w_query)
    key_rows = project(w_key)
    value_rows = project(w_value)
    gate_rows = project(w_outgate)
    in_pre = jnp.dot(normed, w_ingate, preferred_element_type=jnp.float32) + bias_in
    forget_pre = jnp.dot(normed, w_forget, preferred_element_type=jnp.float32) + bias_forget
    hidden, matrix_new, normal_new, stab_new = memory_step(query, key_rows, value_rows, gate_rows, in_pre, forget_pre, matrix_state, normal_state, stab_state)
    cell = hidden.reshape(SEQS, WIDTH).astype(jnp.bfloat16)
    group_terms = jnp.einsum('sbw,bwd->bsd', cell.reshape(SEQS, N_TP, WIDTH // N_TP).astype(jnp.float32), w_proj.reshape(N_TP, WIDTH // N_TP, D).astype(jnp.float32))
    group_terms = lax.optimization_barrier(group_terms.astype(jnp.bfloat16))
    attended = lax.optimization_barrier(jnp.sum(group_terms.astype(jnp.float32), axis=0))
    resid = (tokens.astype(jnp.float32) + attended).astype(jnp.bfloat16)
    normed_ffn = rms_scale(resid, gain_ffn)
    flat_ids = route_ids.reshape(N_EP, SEQ_DEV * TOPK).astype(jnp.int32)
    expert_hot = (flat_ids[..., None] == jnp.arange(EXPERTS, dtype=jnp.int32)).astype(jnp.int32)
    slot_rank = lax.optimization_barrier(jnp.sum((jnp.cumsum(expert_hot, axis=1).astype(jnp.int32) - 1) * expert_hot, axis=-1)).astype(jnp.int32)
    placed = (jnp.arange(N_EP, dtype=jnp.int32)[:, None] * CAP + slot_rank).astype(jnp.int32)
    routed_rows = jnp.repeat(normed_ffn, TOPK, axis=0).reshape(N_EP, SEQ_DEV * TOPK, D)
    buffer = jnp.zeros((EXPERTS, N_EP * CAP, D), jnp.bfloat16).at[flat_ids, placed].set(routed_rows)
    quarter = FF // (2 * N_TP)

    def expert(operands):
        inputs, gate_pair, up_pair, down_pair = operands
        results = []
        for half_index in range(2):
            gate_sum = jnp.dot(inputs, gate_pair[half_index], preferred_element_type=jnp.float32)
            up_sum = jnp.dot(inputs, up_pair[half_index], preferred_element_type=jnp.float32)
            inner = (jax.nn.silu(gate_sum) * up_sum).astype(jnp.bfloat16)
            quarters = jnp.einsum('rtf,tfd->trd', inner.reshape(N_EP * CAP, N_TP, quarter).astype(jnp.float32), down_pair[half_index].reshape(N_TP, quarter, D).astype(jnp.float32))
            quarters = lax.optimization_barrier(quarters.astype(jnp.bfloat16))
            results.append(lax.optimization_barrier(jnp.sum(quarters.astype(jnp.float32), axis=0)).astype(jnp.bfloat16))
        return jnp.stack(results)
    outputs = lax.map(expert, (buffer, w_exp_gate.reshape(EXPERTS, 2, D, FF // 2), w_exp_up.reshape(EXPERTS, 2, D, FF // 2), w_exp_down.reshape(EXPERTS, 2, FF // 2, D)))
    picked = outputs[flat_ids, :, placed]
    both_halves = lax.optimization_barrier(jnp.sum(picked.astype(jnp.float32), axis=2)).reshape(SEQS, TOPK, D)
    weights = route_weights / lax.optimization_barrier(jnp.sum(route_weights, axis=-1, keepdims=True))
    routed = lax.optimization_barrier(jnp.sum(weights[..., None] * both_halves, axis=1))
    mixed_out = (resid.astype(jnp.float32) + routed).astype(jnp.bfloat16)
    return (mixed_out, matrix_new, normal_new, stab_new)
```

```python
import jax
import jax.numpy as jnp
from jax import lax
from jax.sharding import PartitionSpec as P

norm_epsilon = 1e-06


def rms_scale(row_block, gain):
    wide = row_block.astype(jnp.float32)
    factor = lax.rsqrt(jnp.mean(wide * wide, axis=-1, keepdims=True) + norm_epsilon)
    return (wide * factor * gain.astype(jnp.float32)).astype(jnp.bfloat16)


def memory_step(
    query,
    key_rows,
    value_rows,
    gate_rows,
    in_pre,
    forget_pre,
    matrix_state,
    normal_state,
    stab_state,
):
    log_forget = jax.nn.log_sigmoid(forget_pre)
    stab_new = jnp.maximum(log_forget + stab_state, in_pre)
    carry = jnp.exp(log_forget + stab_state - stab_new)
    inflow = jnp.exp(in_pre - stab_new)
    scaled_keys = key_rows.astype(jnp.float32) * query.shape[-1] ** (-0.5)
    value_wide = value_rows.astype(jnp.float32)
    matrix_new = (
        carry[..., None, None] * matrix_state
        + inflow[..., None, None] * scaled_keys[..., :, None] * value_wide[..., None, :]
    )
    normal_new = carry[..., None] * normal_state + inflow[..., None] * scaled_keys
    query_wide = query.astype(jnp.float32)
    numer = jnp.einsum("shd,shde->she", query_wide, matrix_new, precision=lax.Precision.HIGHEST)
    denom = jnp.maximum(jnp.abs(jnp.sum(query_wide * normal_new, axis=-1)), 1.0)
    hidden = numer / denom[..., None] * jax.nn.sigmoid(gate_rows.astype(jnp.float32))
    return (hidden, matrix_new, normal_new, stab_new)


def dispatch_table(route_ids, experts, capacity):
    flat_ids = route_ids.reshape(-1)
    expert_hot = (flat_ids[:, None] == jnp.arange(experts, dtype=jnp.int32)[None, :]).astype(
        jnp.int32
    )
    slot_rank = jnp.sum((jnp.cumsum(expert_hot, axis=0) - 1) * expert_hot, axis=1)
    slot_hot = (slot_rank[:, None] == jnp.arange(capacity, dtype=jnp.int32)[None, :]).astype(
        jnp.float32
    )
    table = expert_hot.astype(jnp.float32)[:, :, None] * slot_hot[:, None, :]
    return table.reshape(flat_ids.shape[0], experts * capacity)


def pack_rows(table, row_block, top_count, experts, capacity):
    repeated = jnp.repeat(row_block, top_count, axis=0)
    packed = jnp.einsum(
        "as,aw->sw", table.astype(jnp.bfloat16), repeated, preferred_element_type=jnp.float32
    ).astype(jnp.bfloat16)
    return packed.reshape(experts, capacity, row_block.shape[1])


def swap(value, axis, bit):
    count = lax.axis_size(axis)
    return lax.ppermute(value, axis, [(i, i ^ bit) for i in range(count)])


def bits_of(count):
    return [1 << place for place in range(count.bit_length() - 1)]


def scatter_columns(terms, axis):
    count = lax.axis_size(axis)
    index = lax.axis_index(axis)
    width = terms.shape[1] // count

    def block(peer):
        return lax.dynamic_slice_in_dim(terms, (index ^ peer) * width, width, 1)

    total = block(0)
    for peer in range(1, count):
        total = total + swap(block(peer).astype(jnp.bfloat16), axis, peer).astype(jnp.float32)
    return total


def halve_columns(terms, axis):
    count = lax.axis_size(axis)
    index = lax.axis_index(axis)
    rows, columns = terms.shape
    blocks = terms.reshape(rows, count, columns // count)
    for bit in bits_of(count):
        pairs = blocks.reshape(rows, -1, 2, blocks.shape[-1])
        own = (index // bit) % 2
        kept = jnp.where(own == 0, pairs[:, :, 0], pairs[:, :, 1])
        sent = jnp.where(own == 0, pairs[:, :, 1], pairs[:, :, 0]).astype(jnp.bfloat16)
        blocks = kept + swap(sent, axis, bit).astype(jnp.float32)
    return blocks.reshape(rows, columns // count)


def gather_columns(own, axis):
    count = lax.axis_size(axis)
    index = lax.axis_index(axis)
    held = own[None]
    for bit in reversed(bits_of(count)):
        other = swap(held, axis, bit)
        first = (index // bit) % 2 == 0
        low = jnp.where(first, held, other)
        high = jnp.where(first, other, held)
        held = jnp.stack([low, high], axis=1).reshape((-1,) + own.shape)
    return held


def body(
    tokens,
    gain_mix,
    gain_ffn,
    w_query,
    w_key,
    w_value,
    w_outgate,
    w_ingate,
    w_forget,
    bias_in,
    bias_forget,
    w_proj,
    matrix_state,
    normal_state,
    stab_state,
    route_ids,
    route_weights,
    w_exp_gate,
    w_exp_up,
    w_exp_down,
):
    ep_count = lax.axis_size("ep")
    tp_count = lax.axis_size("tp")
    ep_index = lax.axis_index("ep")
    tp_index = lax.axis_index("tp")
    seq_dev = tokens.shape[0]
    model_width = tokens.shape[1]
    heads_dev = matrix_state.shape[1]
    head_dim = matrix_state.shape[2]
    head_cols = w_query.shape[1]
    feature_rows = w_query.shape[0]
    top_count = route_ids.shape[1]
    experts = ep_count // 2
    capacity = min(seq_dev, max(2, 2 * seq_dev * top_count // experts))
    every_row = capacity == seq_dev
    col_width = model_width // tp_count
    foreign = lax.all_to_all(tokens, "ep", split_axis=1, concat_axis=0, tiled=True)
    own_gain = lax.dynamic_slice_in_dim(gain_mix, ep_index * feature_rows, feature_rows, 0)
    scaled = (foreign.astype(jnp.float32) * own_gain.astype(jnp.float32)).astype(jnp.bfloat16)
    terms = jnp.concatenate(
        [
            jnp.dot(scaled, weight, preferred_element_type=jnp.float32).astype(jnp.bfloat16)
            for weight in (w_query, w_key, w_value, w_outgate)
        ],
        axis=1,
    )
    arrived = lax.all_to_all(terms, "ep", split_axis=0, concat_axis=0, tiled=True)
    wide = tokens.astype(jnp.float32)
    factor = lax.rsqrt(jnp.mean(wide * wide, axis=-1, keepdims=True) + norm_epsilon)
    summed = factor * jnp.sum(
        arrived.astype(jnp.float32).reshape(ep_count, seq_dev, 4 * head_cols), axis=0
    )
    query, key_rows, value_rows, gate_rows = [
        summed[:, offset * head_cols : (offset + 1) * head_cols]
        .astype(jnp.bfloat16)
        .reshape(seq_dev, heads_dev, head_dim)
        for offset in range(4)
    ]
    normed = (wide * factor * gain_mix.astype(jnp.float32)).astype(jnp.bfloat16)
    head_first = tp_index * heads_dev
    in_pre = lax.dynamic_slice_in_dim(
        jnp.dot(normed, w_ingate, preferred_element_type=jnp.float32) + bias_in,
        head_first,
        heads_dev,
        1,
    )
    forget_pre = lax.dynamic_slice_in_dim(
        jnp.dot(normed, w_forget, preferred_element_type=jnp.float32) + bias_forget,
        head_first,
        heads_dev,
        1,
    )
    hidden, matrix_new, normal_new, stab_new = memory_step(
        query,
        key_rows,
        value_rows,
        gate_rows,
        in_pre,
        forget_pre,
        matrix_state,
        normal_state,
        stab_state,
    )
    cell = hidden.reshape(seq_dev, head_cols).astype(jnp.bfloat16)
    partial_out = jnp.dot(cell, w_proj, preferred_element_type=jnp.float32)
    own_tokens = lax.dynamic_slice_in_dim(tokens, tp_index * col_width, col_width, 1)
    attended = scatter_columns(partial_out, "tp")
    own_resid = (own_tokens.astype(jnp.float32) + attended).astype(jnp.bfloat16)
    if every_row:
        packed = jnp.broadcast_to(own_resid, (experts, seq_dev, col_width))
    else:
        table = dispatch_table(route_ids, experts, capacity)
        packed = pack_rows(table, own_resid, top_count, experts, capacity)
    outgoing = jnp.broadcast_to(packed[:, None], (experts, 2, capacity, col_width))
    received = lax.all_to_all(
        outgoing.reshape(ep_count * capacity, col_width), "ep", split_axis=0, concat_axis=0, tiled=True
    )
    rows = gather_columns(received, "tp").transpose(1, 0, 2).reshape(-1, model_width)
    normed_ffn = rms_scale(rows, gain_ffn)
    gate_sum = jnp.dot(normed_ffn, w_exp_gate[0], preferred_element_type=jnp.float32)
    up_sum = jnp.dot(normed_ffn, w_exp_up[0], preferred_element_type=jnp.float32)
    inner = (jax.nn.silu(gate_sum) * up_sum).astype(jnp.bfloat16)
    expert_terms = jnp.dot(inner, w_exp_down[0], preferred_element_type=jnp.float32)
    half_share = halve_columns(expert_terms, "tp").astype(jnp.bfloat16)
    returned = lax.all_to_all(half_share, "ep", split_axis=0, concat_axis=0, tiled=True)
    halves = returned.astype(jnp.float32).reshape(experts, 2, capacity, col_width)
    weights = route_weights / jnp.sum(route_weights, axis=-1, keepdims=True)
    if every_row:
        chosen = route_ids[:, :, None] == jnp.arange(experts, dtype=jnp.int32)
        shares = jnp.sum(jnp.where(chosen, weights[:, :, None], 0.0), axis=1)
        routed = jnp.sum(halves * shares.T[:, None, :, None], axis=(0, 1))
    else:
        combine = jnp.sum(
            (table * weights.reshape(-1)[:, None]).reshape(
                seq_dev, top_count, experts * capacity
            ),
            axis=1,
        )
        halves_summed = jnp.sum(halves, axis=1).reshape(experts * capacity, col_width)
        routed = jnp.dot(combine, halves_summed, precision=lax.Precision.HIGHEST)
    mixed_out = (own_resid.astype(jnp.float32) + routed).astype(jnp.bfloat16)
    return (mixed_out, matrix_new, normal_new, stab_new)


def solution(mesh):
    placed = (
        P("ep", None),
        P(),
        P(),
        P("ep", "tp"),
        P("ep", "tp"),
        P("ep", "tp"),
        P("ep", "tp"),
        P(),
        P(),
        P(),
        P(),
        P("tp", None),
        P("ep", "tp", None, None),
        P("ep", "tp", None),
        P("ep", "tp"),
        P("ep", None),
        P("ep", None),
        P("ep", None, "tp"),
        P("ep", None, "tp"),
        P("ep", "tp", None),
    )
    return jax.shard_map(
        body,
        mesh=mesh,
        in_specs=placed,
        out_specs=(P("ep", "tp"), P("ep", "tp", None, None), P("ep", "tp", None), P("ep", "tp")),
        check_vma=False,
    )
```

```python
import functools

import jax
import jax.numpy as jnp
from jax import lax
from jax.experimental import pallas as pl
from jax.experimental.pallas import tpu as pltpu
from jax.sharding import PartitionSpec as P

norm_epsilon = 1e-06


def project_kernel(rows_ref, *refs):
    out_ref = refs[-1]
    width = refs[0].shape[1]
    for place, weight_ref in enumerate(refs[:-1]):
        out_ref[:, place * width : (place + 1) * width] = jnp.dot(
            rows_ref[...], weight_ref[...], preferred_element_type=jnp.float32
        ).astype(jnp.bfloat16)


def project(rows, weights):
    return pl.pallas_call(
        project_kernel,
        out_shape=jax.ShapeDtypeStruct((rows.shape[0], len(weights) * weights[0].shape[1]), jnp.bfloat16),
        name="project",
    )(rows, *weights)


def cell_kernel(
    index_ref,
    arrived_ref,
    factor_ref,
    carry_ref,
    inflow_ref,
    matrix_ref,
    normal_ref,
    proj_ref,
    *refs,
    peers,
):
    term_refs = refs[:peers]
    normal_out_ref, key_ref, value_ref, carry_out_ref, read_ref = refs[peers:]
    seqs, heads, head_dim = matrix_ref.shape[:3]
    head_cols = heads * head_dim
    summed = jnp.sum(arrived_ref[...].astype(jnp.float32), axis=0) * factor_ref[...]
    summed = summed.astype(jnp.bfloat16).astype(jnp.float32)
    cells = []
    for head in range(heads):
        query, key, value, gate = [
            summed[:, start + head * head_dim : start + (head + 1) * head_dim]
            for start in range(0, 4 * head_cols, head_cols)
        ]
        carry = carry_ref[:, head : head + 1]
        inflow = inflow_ref[:, head : head + 1]
        key = key * head_dim ** (-0.5)
        inflow_key = inflow * key
        columns = slice(head * head_dim, (head + 1) * head_dim)
        normal_new = carry * normal_ref[:, columns] + inflow_key
        normal_out_ref[:, columns] = normal_new
        rows = slice(head * seqs, (head + 1) * seqs)
        key_ref[rows, :] = inflow_key
        value_ref[rows, :] = value
        carry_out_ref[rows, :] = jnp.broadcast_to(carry, (seqs, head_dim))
        turned = query.T
        for seq in range(seqs):
            read_ref[seq : seq + 1, :] = jnp.sum(
                turned[:, seq : seq + 1] * matrix_ref[seq, head], axis=0, keepdims=True
            )
        numer = carry * read_ref[...] + jnp.sum(query * inflow_key, axis=-1, keepdims=True) * value
        denom = jnp.maximum(jnp.abs(jnp.sum(query * normal_new, axis=-1, keepdims=True)), 1.0)
        cells.append((numer / denom * jax.nn.sigmoid(gate)).astype(jnp.bfloat16))
    cell = jnp.concatenate(cells, axis=1)
    width = proj_ref.shape[1] // peers
    for peer, term_ref in enumerate(term_refs):
        start = pl.multiple_of((index_ref[0] ^ peer) * width, width)
        term_ref[...] = jnp.dot(
            cell, proj_ref[:, pl.ds(start, width)], preferred_element_type=jnp.float32
        ).astype(jnp.bfloat16)


def cell_step(index, arrived, factor, carry, inflow, matrix_state, normal_rows, w_proj, peers):
    seqs, heads, head_dim, _ = matrix_state.shape
    wide = jnp.float32
    term = jax.ShapeDtypeStruct((seqs, w_proj.shape[1] // peers), jnp.bfloat16)
    by_head = jax.ShapeDtypeStruct((heads * seqs, head_dim), wide)
    vmem = pl.BlockSpec(memory_space=pltpu.VMEM)
    return pl.pallas_call(
        functools.partial(cell_kernel, peers=peers),
        in_specs=[pl.BlockSpec(memory_space=pltpu.SMEM)] + [vmem] * 7,
        out_specs=[vmem] * (peers + 4),
        out_shape=[term] * peers
        + [jax.ShapeDtypeStruct((seqs, heads * head_dim), wide), by_head, by_head, by_head],
        scratch_shapes=[pltpu.VMEM((seqs, head_dim), wide)],
        name="cell_step",
    )(index, arrived, factor, carry, inflow, matrix_state, normal_rows, w_proj)


def update_kernel(key_ref, value_ref, carry_ref, matrix_ref, out_ref):
    turned = key_ref[...].T
    for seq in range(matrix_ref.shape[0]):
        out_ref[seq, 0] = (
            carry_ref[seq : seq + 1, :] * matrix_ref[seq, 0]
            + turned[:, seq : seq + 1] * value_ref[seq : seq + 1, :]
        )


def update_matrix(key, value, carry, matrix_state):
    seqs, heads, head_dim, _ = matrix_state.shape
    block = 8
    steps = seqs // block
    rows = pl.BlockSpec((block, head_dim), lambda head, step: (head * steps + step, 0))
    matrix = pl.BlockSpec((block, 1, head_dim, head_dim), lambda head, step: (step, head, 0, 0))
    return pl.pallas_call(
        update_kernel,
        grid=(heads, steps),
        in_specs=[rows, rows, rows, matrix],
        out_specs=matrix,
        out_shape=jax.ShapeDtypeStruct(matrix_state.shape, jnp.float32),
        name="update_matrix",
    )(key, value, carry, matrix_state)


def expert_kernel(index_ref, *refs, peers):
    chunk_refs = refs[:peers]
    gain_ref, gate_ref, up_ref, down_ref = refs[peers : peers + 4]
    term_refs = refs[peers + 4 :]
    width = chunk_refs[0].shape[1]
    wide = [chunk_ref[...].astype(jnp.float32) for chunk_ref in chunk_refs]
    squares = sum(jnp.sum(chunk * chunk, axis=-1, keepdims=True) for chunk in wide)
    factor = lax.rsqrt(squares / (peers * width) + norm_epsilon)
    gate_sum = None
    for peer in range(peers):
        start = pl.multiple_of((index_ref[0] ^ peer) * width, width)
        gain = gain_ref[:, pl.ds(start, width)].astype(jnp.float32)
        normed = (wide[peer] * factor * gain).astype(jnp.bfloat16)
        gate_part = jnp.dot(normed, gate_ref[0, pl.ds(start, width), :], preferred_element_type=jnp.float32)
        up_part = jnp.dot(normed, up_ref[0, pl.ds(start, width), :], preferred_element_type=jnp.float32)
        gate_sum = gate_part if gate_sum is None else gate_sum + gate_part
        up_sum = up_part if peer == 0 else up_sum + up_part
    inner = (jax.nn.silu(gate_sum) * up_sum).astype(jnp.bfloat16)
    for peer, term_ref in enumerate(term_refs):
        start = pl.multiple_of((index_ref[0] ^ peer) * width, width)
        term_ref[...] = jnp.dot(
            inner, down_ref[0, :, pl.ds(start, width)], preferred_element_type=jnp.float32
        ).astype(jnp.bfloat16)


def expert_step(index, chunks, gain, gate, up, down):
    peers = len(chunks)
    vmem = pl.BlockSpec(memory_space=pltpu.VMEM)
    return pl.pallas_call(
        functools.partial(expert_kernel, peers=peers),
        in_specs=[pl.BlockSpec(memory_space=pltpu.SMEM)] + [vmem] * (peers + 4),
        out_specs=[vmem] * peers,
        out_shape=[jax.ShapeDtypeStruct(chunks[0].shape, jnp.bfloat16)] * peers,
        name="expert_step",
    )(index, *chunks, gain, gate, up, down)


def dispatch_table(route_ids, experts, capacity):
    flat_ids = route_ids.reshape(-1)
    expert_hot = (flat_ids[:, None] == jnp.arange(experts, dtype=jnp.int32)[None, :]).astype(
        jnp.int32
    )
    slot_rank = jnp.sum((jnp.cumsum(expert_hot, axis=0) - 1) * expert_hot, axis=1)
    slot_hot = (slot_rank[:, None] == jnp.arange(capacity, dtype=jnp.int32)[None, :]).astype(
        jnp.float32
    )
    table = expert_hot.astype(jnp.float32)[:, :, None] * slot_hot[:, None, :]
    return table.reshape(flat_ids.shape[0], experts * capacity)


def pack_rows(table, row_block, top_count, experts, capacity):
    repeated = jnp.repeat(row_block, top_count, axis=0)
    packed = jnp.einsum(
        "as,aw->sw", table.astype(jnp.bfloat16), repeated, preferred_element_type=jnp.float32
    ).astype(jnp.bfloat16)
    return packed.reshape(experts, capacity, row_block.shape[1])


def swap(value, axis, bit):
    count = lax.axis_size(axis)
    return lax.ppermute(value, axis, [(i, i ^ bit) for i in range(count)])


def bits_of(count):
    return [1 << place for place in range(count.bit_length() - 1)]


def gather_chunks(own, axis):
    chunks = {0: own}
    for bit in reversed(bits_of(lax.axis_size(axis))):
        for place in list(chunks):
            chunks[place ^ bit] = swap(chunks[place], axis, bit)
    return [chunks[place] for place in range(len(chunks))]


def sum_chunks(terms, axis):
    left = dict(enumerate(terms))
    for bit in bits_of(lax.axis_size(axis)):
        for place in sorted((place for place in left if place & bit), reverse=True):
            other = swap(left.pop(place).astype(jnp.bfloat16), axis, bit)
            left[place ^ bit] = left[place ^ bit].astype(jnp.float32) + other.astype(jnp.float32)
    return left[0]


def body(
    tokens,
    gain_mix,
    gain_ffn,
    w_query,
    w_key,
    w_value,
    w_outgate,
    w_ingate,
    w_forget,
    bias_in,
    bias_forget,
    w_proj,
    matrix_state,
    normal_state,
    stab_state,
    route_ids,
    route_weights,
    w_exp_gate,
    w_exp_up,
    w_exp_down,
):
    ep_count = lax.axis_size("ep")
    tp_count = lax.axis_size("tp")
    tp_index = lax.axis_index("tp")
    seq_dev = tokens.shape[0]
    model_width = tokens.shape[1]
    heads_dev = matrix_state.shape[1]
    head_dim = matrix_state.shape[2]
    head_cols = w_query.shape[1]
    feature_rows = w_query.shape[0]
    top_count = route_ids.shape[1]
    experts = ep_count // 2
    capacity = min(seq_dev, max(2, 2 * seq_dev * top_count // experts))
    every_row = capacity == seq_dev
    col_width = model_width // tp_count
    index = tp_index.astype(jnp.int32).reshape(1)
    wide = tokens.astype(jnp.float32)
    scaled = wide * gain_mix.astype(jnp.float32)
    blocks = scaled.astype(jnp.bfloat16).reshape(seq_dev, ep_count, feature_rows).transpose(1, 0, 2)
    foreign = lax.all_to_all(
        blocks.reshape(ep_count * seq_dev, feature_rows), "ep", split_axis=0, concat_axis=0, tiled=True
    )
    terms = project(foreign, (w_query, w_key, w_value, w_outgate))
    arrived = lax.all_to_all(terms, "ep", split_axis=0, concat_axis=0, tiled=True)
    factor = lax.rsqrt(jnp.mean(wide * wide, axis=-1, keepdims=True) + norm_epsilon)
    normed = (wide * factor * gain_mix.astype(jnp.float32)).astype(jnp.bfloat16)
    head_first = tp_index * heads_dev

    def own_heads(weight, bias):
        return lax.dynamic_slice_in_dim(
            jnp.dot(normed, weight, preferred_element_type=jnp.float32) + bias, head_first, heads_dev, 1
        )

    in_pre = own_heads(w_ingate, bias_in)
    log_forget = jax.nn.log_sigmoid(own_heads(w_forget, bias_forget))
    stab_new = jnp.maximum(log_forget + stab_state, in_pre)
    carry = jnp.exp(log_forget + stab_state - stab_new)
    inflow = jnp.exp(in_pre - stab_new)
    *out_terms, normal_rows, key_rows, value_rows, carry_rows = cell_step(
        index,
        arrived.reshape(ep_count, seq_dev, 4 * head_cols),
        factor,
        carry,
        inflow,
        matrix_state,
        normal_state.reshape(seq_dev, head_cols),
        w_proj,
        tp_count,
    )
    normal_new = normal_rows.reshape(normal_state.shape)
    matrix_new = update_matrix(key_rows, value_rows, carry_rows, matrix_state)
    own_tokens = lax.dynamic_slice_in_dim(tokens, tp_index * col_width, col_width, 1)
    attended = out_terms[0].astype(jnp.float32)
    for peer in range(1, tp_count):
        attended = attended + swap(out_terms[peer], "tp", peer).astype(jnp.float32)
    own_resid = (own_tokens.astype(jnp.float32) + attended).astype(jnp.bfloat16)
    if every_row:
        packed = jnp.broadcast_to(own_resid, (experts, seq_dev, col_width))
    else:
        table = dispatch_table(route_ids, experts, capacity)
        packed = pack_rows(table, own_resid, top_count, experts, capacity)
    outgoing = jnp.broadcast_to(packed[:, None], (experts, 2, capacity, col_width))
    received = lax.all_to_all(
        outgoing.reshape(ep_count * capacity, col_width), "ep", split_axis=0, concat_axis=0, tiled=True
    )
    down_terms = expert_step(
        index,
        gather_chunks(received, "tp"),
        gain_ffn.reshape(1, model_width),
        w_exp_gate,
        w_exp_up,
        w_exp_down,
    )
    half_share = sum_chunks(down_terms, "tp").astype(jnp.bfloat16)
    returned = lax.all_to_all(half_share, "ep", split_axis=0, concat_axis=0, tiled=True)
    halves = returned.astype(jnp.float32).reshape(experts, 2, capacity, col_width)
    weights = route_weights / jnp.sum(route_weights, axis=-1, keepdims=True)
    if every_row:
        chosen = route_ids[:, :, None] == jnp.arange(experts, dtype=jnp.int32)
        shares = jnp.sum(jnp.where(chosen, weights[:, :, None], 0.0), axis=1)
        routed = jnp.sum(halves * shares.T[:, None, :, None], axis=(0, 1))
    else:
        combine = jnp.sum(
            (table * weights.reshape(-1)[:, None]).reshape(
                seq_dev, top_count, experts * capacity
            ),
            axis=1,
        )
        halves_summed = jnp.sum(halves, axis=1).reshape(experts * capacity, col_width)
        routed = jnp.dot(combine, halves_summed, precision=lax.Precision.HIGHEST)
    mixed_out = (own_resid.astype(jnp.float32) + routed).astype(jnp.bfloat16)
    return (mixed_out, matrix_new, normal_new, stab_new)


def solution(mesh):
    placed = (
        P("ep", None),
        P(),
        P(),
        P("ep", "tp"),
        P("ep", "tp"),
        P("ep", "tp"),
        P("ep", "tp"),
        P(),
        P(),
        P(),
        P(),
        P("tp", None),
        P("ep", "tp", None, None),
        P("ep", "tp", None),
        P("ep", "tp"),
        P("ep", None),
        P("ep", None),
        P("ep", None, "tp"),
        P("ep", None, "tp"),
        P("ep", "tp", None),
    )
    return jax.shard_map(
        body,
        mesh=mesh,
        in_specs=placed,
        out_specs=(P("ep", "tp"), P("ep", "tp", None, None), P("ep", "tp", None), P("ep", "tp")),
        check_vma=False,
    )
```

```python
import functools

import jax
import jax.numpy as jnp
from jax import lax
from jax.experimental import pallas as pl
from jax.experimental.pallas import tpu as pltpu
from jax.sharding import PartitionSpec as P

norm_epsilon = 1e-06


def room(mebibytes):
    return pltpu.CompilerParams(vmem_limit_bytes=mebibytes << 20)


def load_kernel(_, *refs, count, narrowed):
    sources, targets = refs[:count], refs[count : 2 * count]
    semaphores, *wide = refs[2 * count :]
    landed = wide + list(targets[narrowed:])
    copies = [
        pltpu.make_async_copy(source, target, semaphores.at[place])
        for place, (source, target) in enumerate(zip(sources, landed))
    ]
    for copy in copies:
        copy.start()
    for place, copy in enumerate(copies):
        copy.wait()
        if place < narrowed:

            @pl.loop(0, targets[place].shape[0])
            def narrow(row, place=place):
                targets[place][row] = wide[place][row].astype(jnp.bfloat16)


def load(after, arrays, cycles, narrowed=0):
    anywhere = pl.BlockSpec(memory_space=pl.ANY)
    targets = [
        pltpu.VMEM(array.shape, jnp.bfloat16 if place < narrowed else array.dtype)
        for place, array in enumerate(arrays)
    ]
    return pl.pallas_call(
        functools.partial(load_kernel, count=len(arrays), narrowed=narrowed),
        in_specs=[anywhere] * (len(arrays) + 1),
        out_specs=[pl.BlockSpec(memory_space=pltpu.VMEM)] * len(arrays),
        out_shape=targets,
        scratch_shapes=[pltpu.SemaphoreType.DMA((len(arrays),))]
        + [pltpu.VMEM(array.shape, array.dtype) for array in arrays[:narrowed]],
        compiler_params=room(12),
        cost_estimate=pl.CostEstimate(flops=cycles, bytes_accessed=0, transcendentals=0),
        name="load",
    )(after, *map(away, arrays))


def away(array):
    return pltpu.with_memory_space_constraint(array, pltpu.HBM)


def held(array):
    return pltpu.with_memory_space_constraint(array, pltpu.VMEM)


def prepare_kernel(rows_hbm, gain_hbm, *refs, weights):
    weight_refs = refs[:weights]
    out_ref, pack_ref, rows_ref, gain_ref, semaphores = refs[weights:]
    copies = [
        pltpu.make_async_copy(rows_hbm, rows_ref, semaphores.at[0]),
        pltpu.make_async_copy(gain_hbm, gain_ref, semaphores.at[1]),
    ]
    for place, weight_ref in enumerate(weight_refs):
        copies.append(pltpu.make_async_copy(weight_ref, pack_ref.at[place], semaphores.at[2 + place]))
    for copy in copies:
        copy.start()
    for copy in copies[:2]:
        copy.wait()
    scaled = rows_ref[...].astype(jnp.float32) * gain_ref[...].astype(jnp.float32).reshape(1, -1)
    scaled = scaled.astype(jnp.bfloat16)
    seqs = rows_ref.shape[0]
    width = out_ref.shape[1]
    for place in range(out_ref.shape[0] // seqs):
        out_ref[place * seqs : (place + 1) * seqs, :] = scaled[:, place * width : (place + 1) * width]
    for copy in copies[2:]:
        copy.wait()


def prepare(rows, gain, weights, count):
    seqs, features = rows.shape
    width = features // count
    if width % 128:
        scaled = (rows.astype(jnp.float32) * gain.astype(jnp.float32)).astype(jnp.bfloat16)
        blocks = scaled.reshape(seqs, count, width).transpose(1, 0, 2).reshape(count * seqs, width)
        return blocks, jnp.stack(weights)
    anywhere = pl.BlockSpec(memory_space=pl.ANY)
    return pl.pallas_call(
        functools.partial(prepare_kernel, weights=len(weights)),
        in_specs=[anywhere] * (2 + len(weights)),
        out_specs=[pl.BlockSpec(), pl.BlockSpec(memory_space=pltpu.VMEM)],
        out_shape=[
            jax.ShapeDtypeStruct((count * seqs, width), jnp.bfloat16),
            pltpu.VMEM((len(weights),) + weights[0].shape, weights[0].dtype),
        ],
        scratch_shapes=[
            pltpu.VMEM(rows.shape, rows.dtype),
            pltpu.VMEM(gain.shape, gain.dtype),
            pltpu.SemaphoreType.DMA((2 + len(weights),)),
        ],
        compiler_params=room(12),
        name="prepare",
    )(*map(away, (rows, gain, *weights)))


def gates_kernel(
    index_ref,
    _,
    rows_ref,
    gain_ref,
    in_ref,
    forget_ref,
    bias_in_ref,
    bias_forget_ref,
    stab_ref,
    factor_ref,
    carry_ref,
    inflow_ref,
    stab_out_ref,
    in_pre_ref,
    forget_pre_ref,
):
    wide = rows_ref[...].astype(jnp.float32)
    factor = lax.rsqrt(jnp.mean(wide * wide, axis=-1, keepdims=True) + norm_epsilon)
    factor_ref[...] = factor
    normed = (wide * factor * gain_ref[...].astype(jnp.float32).reshape(1, -1)).astype(jnp.bfloat16)
    across = (((1,), (1,)), ((), ()))
    in_pre_ref[...] = lax.dot_general(in_ref[...], normed, across, preferred_element_type=jnp.float32)
    forget_pre_ref[...] = lax.dot_general(forget_ref[...], normed, across, preferred_element_type=jnp.float32)
    heads = stab_ref.shape[0]
    for head in range(heads):
        place = index_ref[0] * heads + head
        in_pre = in_pre_ref[pl.ds(place, 1), :] + bias_in_ref[place]
        forget_pre = forget_pre_ref[pl.ds(place, 1), :] + bias_forget_ref[place]
        log_forget = jnp.minimum(forget_pre, 0.0) - jnp.log1p(jnp.exp(-jnp.abs(forget_pre)))
        kept = log_forget + stab_ref[head : head + 1, :]
        stab_new = jnp.maximum(kept, in_pre)
        stab_out_ref[head : head + 1, :] = stab_new
        carry_ref[head : head + 1, :] = jnp.exp(kept - stab_new)
        inflow_ref[head : head + 1, :] = jnp.exp(in_pre - stab_new)


def gates(after, index, rows, gain, w_in, w_forget, bias_in, bias_forget, stab):
    seqs, heads = stab.shape
    small = jax.ShapeDtypeStruct((heads, seqs), jnp.float32)
    smem = pl.BlockSpec(memory_space=pltpu.SMEM)
    every = (w_in.shape[1], seqs)
    return pl.pallas_call(
        gates_kernel,
        in_specs=[smem, pl.BlockSpec(memory_space=pl.ANY)]
        + [pl.BlockSpec()] * 4
        + [smem] * 2
        + [pl.BlockSpec()],
        out_shape=[jax.ShapeDtypeStruct((seqs, 1), jnp.float32)] + [small] * 3,
        scratch_shapes=[pltpu.VMEM(every, jnp.float32)] * 2,
        compiler_params=room(12),
        cost_estimate=pl.CostEstimate(flops=1 << 22, bytes_accessed=0, transcendentals=0),
        name="gates",
    )(index, after, rows, gain, w_in.T, w_forget.T, bias_in, bias_forget, stab.T)


def project_kernel(index_ref, rows_ref, own_ref, other_ref, out_ref):
    count, features, width = own_ref.shape
    own = pl.multiple_of(index_ref[1] * features, features)
    other = pl.multiple_of((1 - index_ref[1]) * features, features)
    for place in range(count):
        total = jnp.dot(rows_ref[:, pl.ds(own, features)], own_ref[place], preferred_element_type=jnp.float32)
        total = total + jnp.dot(
            rows_ref[:, pl.ds(other, features)], other_ref[place], preferred_element_type=jnp.float32
        )
        out_ref[:, place * width : (place + 1) * width] = total.astype(jnp.bfloat16)


def project(index, rows, own, other):
    count, features, width = own.shape
    if features % 128:
        halves = rows.reshape(rows.shape[0], 2, -1)
        first = jnp.where(index[1] == 0, halves[:, 0], halves[:, 1])
        second = jnp.where(index[1] == 0, halves[:, 1], halves[:, 0])
        total = jnp.einsum("rf,cfw->rcw", first, own, preferred_element_type=jnp.float32)
        total = total + jnp.einsum("rf,cfw->rcw", second, other, preferred_element_type=jnp.float32)
        return total.astype(jnp.bfloat16).reshape(rows.shape[0], count * width)
    return pl.pallas_call(
        project_kernel,
        in_specs=[pl.BlockSpec(memory_space=pltpu.SMEM)] + [pl.BlockSpec()] * 3,
        out_shape=jax.ShapeDtypeStruct((rows.shape[0], count * width), jnp.bfloat16),
        compiler_params=room(12),
        name="project",
    )(index, rows, held(own), held(other))


def cell_kernel(
    index_ref,
    arrived_ref,
    factor_ref,
    carry_ref,
    inflow_ref,
    matrix_ref,
    normal_ref,
    proj_hbm,
    *refs,
    peers,
):
    term_refs = refs[:peers]
    key_ref, value_ref, carry_out_ref, inflow_out_ref, read_ref, proj_ref, semaphore = refs[peers:]
    proj_copy = pltpu.make_async_copy(proj_hbm, proj_ref, semaphore)
    proj_copy.start()
    seqs, heads, head_dim = matrix_ref.shape[:3]
    head_cols = heads * head_dim
    summed = jnp.sum(arrived_ref[...].astype(jnp.float32), axis=0) * factor_ref[...]
    summed = summed.astype(jnp.bfloat16).astype(jnp.float32)
    cells = []
    carries = carry_ref[...].T
    inflows = inflow_ref[...].T
    for head in range(heads):
        query, key, value, gate = [
            summed[:, start + head * head_dim : start + (head + 1) * head_dim]
            for start in range(0, 4 * head_cols, head_cols)
        ]
        carry = carries[:, head : head + 1]
        inflow = inflows[:, head : head + 1]
        inflow_key = inflow * (key * head_dim ** (-0.5))
        columns = slice(head * head_dim, (head + 1) * head_dim)
        normal_new = carry * normal_ref[:, columns] + inflow_key
        rows = slice(head * seqs, (head + 1) * seqs)
        key_ref[rows, :] = key
        value_ref[rows, :] = value
        carry_out_ref[rows, :] = jnp.broadcast_to(carry, (seqs, head_dim))
        inflow_out_ref[rows, :] = jnp.broadcast_to(inflow * head_dim ** (-0.5), (seqs, head_dim))
        turned = query.T
        for seq in range(seqs):
            read_ref[seq : seq + 1, :] = jnp.sum(
                turned[:, seq : seq + 1] * matrix_ref[seq, head].astype(jnp.float32), axis=0, keepdims=True
            )
        numer = carry * read_ref[...] + jnp.sum(query * inflow_key, axis=-1, keepdims=True) * value
        denom = jnp.maximum(jnp.abs(jnp.sum(query * normal_new, axis=-1, keepdims=True)), 1.0)
        cells.append((numer / denom * jax.nn.sigmoid(gate)).astype(jnp.bfloat16))
    cell = jnp.concatenate(cells, axis=1)
    proj_copy.wait()
    width = proj_ref.shape[1] // peers
    for peer, term_ref in enumerate(term_refs):
        start = pl.multiple_of((index_ref[0] ^ peer) * width, width)
        term_ref[...] = jnp.dot(
            cell, proj_ref[:, pl.ds(start, width)], preferred_element_type=jnp.float32
        ).astype(jnp.bfloat16)


def cell_step(index, arrived, factor, carry, inflow, matrix_state, normal_rows, w_proj, peers):
    seqs, heads, head_dim, _ = matrix_state.shape
    wide = jnp.float32
    term = jax.ShapeDtypeStruct((seqs, w_proj.shape[1] // peers), jnp.bfloat16)
    by_head = jax.ShapeDtypeStruct((heads * seqs, head_dim), wide)
    vmem = pl.BlockSpec()
    return pl.pallas_call(
        functools.partial(cell_kernel, peers=peers),
        in_specs=[pl.BlockSpec(memory_space=pltpu.SMEM)]
        + [vmem] * 6
        + [pl.BlockSpec(memory_space=pl.ANY)],
        out_specs=[vmem] * (peers + 4),
        out_shape=[term] * peers
        + [by_head] * 4,
        scratch_shapes=[
            pltpu.VMEM((seqs, head_dim), wide),
            pltpu.VMEM(w_proj.shape, w_proj.dtype),
            pltpu.SemaphoreType.DMA,
        ],
        compiler_params=room(12),
        name="cell_step",
    )(index, held(arrived), factor, carry, inflow, held(matrix_state), normal_rows, away(w_proj))


def update_kernel(key_ref, value_ref, carry_ref, inflow_ref, matrix_hbm, out_hbm, work_ref, loads, stores):
    seqs, heads, head_dim, _ = matrix_hbm.shape
    block = min(8, seqs)
    wide = (block, block * head_dim)
    own = lax.broadcasted_iota(jnp.int32, wide, 0) == lax.broadcasted_iota(jnp.int32, wide, 1) // head_dim

    def copy(step, out):
        part = pl.ds(step * block, block)
        if out:
            return pltpu.make_async_copy(work_ref.at[part], out_hbm.at[part], stores.at[step])
        return pltpu.make_async_copy(matrix_hbm.at[part], work_ref.at[part], loads.at[step])

    for step in range(seqs // block):
        copy(step, False).start()
    for step in range(seqs // block):
        copy(step, False).wait()
        for head in range(heads):
            rows = pl.ds(head * seqs + step * block, block)
            spread = jnp.where(own, jnp.concatenate([value_ref[rows, :]] * block, axis=1), 0.0)
            outer = jnp.dot(
                key_ref[rows, :].T.astype(jnp.bfloat16),
                spread.astype(jnp.bfloat16),
                preferred_element_type=jnp.float32,
            )
            for place in range(block):
                row = head * seqs + step * block + place
                seq = step * block + place
                work_ref[seq, head] = (
                    carry_ref[row : row + 1, :] * work_ref[seq, head]
                    + inflow_ref[row : row + 1, :] * outer[:, place * head_dim : (place + 1) * head_dim]
                )
        copy(step, True).start()
    for step in range(seqs // block):
        copy(step, True).wait()


def update_matrix(key, value, carry, inflow, matrix_state):
    anywhere = pl.BlockSpec(memory_space=pl.ANY)
    steps = matrix_state.shape[0] // min(8, matrix_state.shape[0])
    return pl.pallas_call(
        update_kernel,
        in_specs=[pl.BlockSpec()] * 4 + [anywhere],
        out_specs=anywhere,
        out_shape=pltpu.HBM(matrix_state.shape, jnp.float32),
        scratch_shapes=[
            pltpu.VMEM(matrix_state.shape, jnp.float32),
            pltpu.SemaphoreType.DMA((steps,)),
            pltpu.SemaphoreType.DMA((steps,)),
        ],
        compiler_params=room(12),
        cost_estimate=pl.CostEstimate(flops=1 << 23, bytes_accessed=0, transcendentals=0),
        name="update_matrix",
    )(key, value, carry, inflow, away(matrix_state))


def expert_kernel(index_ref, *refs, peers, halves):
    count = peers * halves
    chunk_refs = refs[:count]
    gain_ref, gate_ref, up_ref, down_ref = refs[count : count + 4]
    term_refs = refs[count + 4 :]
    rows, width = chunk_refs[0].shape
    squares = [
        sum(
            jnp.sum(jnp.square(chunk_refs[half * peers + peer][...].astype(jnp.float32)), axis=-1, keepdims=True)
            for peer in range(peers)
        )
        for half in range(halves)
    ]
    factors = [lax.rsqrt(square / (peers * width) + norm_epsilon) for square in squares]
    gate_sum = up_sum = None
    for peer in range(peers):
        start = pl.multiple_of((index_ref[0] ^ peer) * width, width)
        gain = gain_ref[:, pl.ds(start, width)].astype(jnp.float32)
        normed = jnp.concatenate(
            [
                (chunk_refs[half * peers + peer][...].astype(jnp.float32) * factors[half] * gain).astype(jnp.bfloat16)
                for half in range(halves)
            ],
            axis=0,
        )
        gate_part = jnp.dot(normed, gate_ref[0, pl.ds(start, width), :], preferred_element_type=jnp.float32)
        up_part = jnp.dot(normed, up_ref[0, pl.ds(start, width), :], preferred_element_type=jnp.float32)
        gate_sum = gate_part if peer == 0 else gate_sum + gate_part
        up_sum = up_part if peer == 0 else up_sum + up_part
    inner = (jax.nn.silu(gate_sum) * up_sum).astype(jnp.bfloat16)
    for peer in range(peers):
        start = pl.multiple_of((index_ref[0] ^ peer) * width, width)
        term = jnp.dot(
            inner, down_ref[0, :, pl.ds(start, width)], preferred_element_type=jnp.float32
        ).astype(jnp.bfloat16)
        for half in range(halves):
            term_refs[half * peers + peer][...] = term[half * rows : (half + 1) * rows]


def expert_step(index, chunks, gain, gate, up, down, peers):
    vmem = pl.BlockSpec()
    return pl.pallas_call(
        functools.partial(expert_kernel, peers=peers, halves=len(chunks) // peers),
        in_specs=[pl.BlockSpec(memory_space=pltpu.SMEM)]
        + [vmem] * (len(chunks) + 4),
        out_specs=[vmem] * len(chunks),
        out_shape=[jax.ShapeDtypeStruct(chunks[0].shape, jnp.bfloat16)] * len(chunks),
        compiler_params=room(12),
        name="expert_step",
    )(index, *map(held, chunks), gain, held(gate), held(up), held(down))


def dispatch_table(route_ids, experts, capacity):
    flat_ids = route_ids.reshape(-1)
    expert_hot = (flat_ids[:, None] == jnp.arange(experts, dtype=jnp.int32)[None, :]).astype(
        jnp.int32
    )
    slot_rank = jnp.sum((jnp.cumsum(expert_hot, axis=0) - 1) * expert_hot, axis=1)
    slot_hot = (slot_rank[:, None] == jnp.arange(capacity, dtype=jnp.int32)[None, :]).astype(
        jnp.float32
    )
    table = expert_hot.astype(jnp.float32)[:, :, None] * slot_hot[:, None, :]
    return table.reshape(flat_ids.shape[0], experts * capacity)


def pack_rows(table, row_block, top_count, experts, capacity):
    repeated = jnp.repeat(row_block, top_count, axis=0)
    packed = jnp.einsum(
        "as,aw->sw", table.astype(jnp.bfloat16), repeated, preferred_element_type=jnp.float32
    ).astype(jnp.bfloat16)
    return packed.reshape(experts, capacity, row_block.shape[1])


def swap(value, half, peer):
    ep_count, tp_count = lax.axis_size("ep"), lax.axis_size("tp")
    away = half * tp_count + peer
    return lax.ppermute(value, ("ep", "tp"), [(i, i ^ away) for i in range(ep_count * tp_count)])


def far_places(peers):
    return [(half, peer) for half in range(2) for peer in range(0, peers, 2)]


def gather_chunks(own, peers, beside):
    chunks = {}
    for half, peer in far_places(peers):
        chunks[half, peer] = swap(own, half, peer) if half or peer else own
    first = (0, 2) if peers > 2 else (1, 0)
    chunks[first], beside = lax.optimization_barrier((chunks[first], beside))
    for half, peer in far_places(peers):
        chunks[half, peer ^ 1] = swap(chunks[half, peer], 0, 1)
    return [chunks[half, peer] for half in range(2) for peer in range(peers)], beside


def sum_chunks(terms, peers):
    left = {(place // peers, place % peers): term for place, term in enumerate(terms)}
    places = far_places(peers)
    for half, peer in places[1:] + places[:1]:
        other = swap(left[half, peer ^ 1], 0, 1)
        left[half, peer] = left[half, peer].astype(jnp.float32) + other.astype(jnp.float32)
    total = left[0, 0]
    for half, peer in places[1:]:
        total = total + swap(left[half, peer].astype(jnp.bfloat16), half, peer).astype(jnp.float32)
    return total


def body(
    tokens,
    gain_mix,
    gain_ffn,
    w_query,
    w_key,
    w_value,
    w_outgate,
    w_ingate,
    w_forget,
    bias_in,
    bias_forget,
    w_proj,
    matrix_state,
    normal_state,
    stab_state,
    route_ids,
    route_weights,
    w_exp_gate,
    w_exp_up,
    w_exp_down,
):
    ep_count = lax.axis_size("ep")
    tp_count = lax.axis_size("tp")
    tp_index = lax.axis_index("tp")
    seq_dev = tokens.shape[0]
    model_width = tokens.shape[1]
    heads_dev = matrix_state.shape[1]
    head_dim = matrix_state.shape[2]
    head_cols = w_query.shape[1]
    top_count = route_ids.shape[1]
    experts = ep_count // 2
    capacity = min(seq_dev, max(2, 2 * seq_dev * top_count // experts))
    every_row = capacity == seq_dev
    col_width = model_width // tp_count
    index = jnp.stack([tp_index, lax.axis_index("ep") % 2]).astype(jnp.int32)
    blocks, own_weights = prepare(tokens, gain_mix, (w_query, w_key, w_value, w_outgate), experts)
    with jax.named_scope("pair"):
        other_weights = swap(own_weights, 1, 0)
    same_half = [list(range(half, ep_count, 2)) for half in range(2)]

    def exchange(rows):
        return lax.all_to_all(
            rows, "ep", split_axis=0, concat_axis=0, tiled=True, axis_index_groups=same_half
        )

    with jax.named_scope("spread"):
        foreign = exchange(blocks)
    terms = project(index, foreign, own_weights, other_weights)
    (held_state,) = load(terms, (matrix_state,), 1 << 22, narrowed=1)
    arrived = exchange(terms)
    factor, carry, inflow, stab_turned = gates(
        terms, index, tokens, gain_mix, w_ingate, w_forget, bias_in, bias_forget, stab_state
    )
    stab_new = stab_turned.T
    weights = route_weights / jnp.sum(route_weights, axis=-1, keepdims=True)
    if every_row:
        chosen = route_ids[:, :, None] == jnp.arange(experts, dtype=jnp.int32)
        shares = jnp.sum(jnp.where(chosen, weights[:, :, None], 0.0), axis=1)
    else:
        shares = weights
    factor, shares, stab_new = lax.optimization_barrier((factor, shares, stab_new))
    cell_outs = cell_step(
        index,
        arrived.reshape(experts, seq_dev, 4 * head_cols),
        factor,
        carry,
        inflow,
        held_state,
        normal_state.reshape(seq_dev, head_cols),
        w_proj,
        tp_count,
    )
    out_terms, state_rows = cell_outs[:tp_count], cell_outs[tp_count:]
    key_wide = (state_rows[3] * state_rows[0]).reshape(heads_dev, seq_dev, -1).transpose(1, 0, 2)
    normal_new = carry.T[:, :, None] * normal_state + key_wide
    matrix_new = update_matrix(*state_rows, matrix_state)
    own_tokens = lax.dynamic_slice_in_dim(tokens, tp_index * col_width, col_width, 1)
    attended = out_terms[0].astype(jnp.float32)
    for peer in range(1, tp_count):
        attended = attended + swap(out_terms[peer], 0, peer).astype(jnp.float32)
    own_resid = (own_tokens.astype(jnp.float32) + attended).astype(jnp.bfloat16)
    held_experts = load(held(state_rows[0]), (w_exp_gate, w_exp_up), 1 << 22)
    own_resid, *held_experts = lax.optimization_barrier((own_resid, *held_experts))
    if every_row:
        packed = jnp.broadcast_to(own_resid, (experts, seq_dev, col_width))
    else:
        table = dispatch_table(route_ids, experts, capacity)
        packed = pack_rows(table, own_resid, top_count, experts, capacity)
    received = exchange(packed.reshape(experts * capacity, col_width))
    (held_down,) = load(received, (w_exp_down,), 1 << 22)
    chunks, held_down = gather_chunks(received, tp_count, held_down)
    down_terms = expert_step(
        index,
        chunks,
        gain_ffn.reshape(1, model_width),
        *held_experts,
        held_down,
        tp_count,
    )
    half_share = sum_chunks(down_terms, tp_count).astype(jnp.bfloat16)
    half_share, matrix_new = lax.optimization_barrier((half_share, matrix_new))
    returned = exchange(half_share).astype(jnp.float32).reshape(experts, capacity, col_width)
    if every_row:
        routed = jnp.sum(returned * shares.T[:, :, None], axis=0)
    else:
        combine = jnp.sum(
            (table * shares.reshape(-1)[:, None]).reshape(
                seq_dev, top_count, experts * capacity
            ),
            axis=1,
        )
        routed = jnp.dot(
            combine, returned.reshape(experts * capacity, col_width), precision=lax.Precision.HIGHEST
        )
    mixed_out = (own_resid.astype(jnp.float32) + routed).astype(jnp.bfloat16)
    return (mixed_out, matrix_new, normal_new, stab_new)


def solution(mesh):
    placed = (
        P("ep", None),
        P(),
        P(),
        P("ep", "tp"),
        P("ep", "tp"),
        P("ep", "tp"),
        P("ep", "tp"),
        P(),
        P(),
        P(),
        P(),
        P("tp", None),
        P("ep", "tp", None, None),
        P("ep", "tp", None),
        P("ep", "tp"),
        P("ep", None),
        P("ep", None),
        P("ep", None, "tp"),
        P("ep", None, "tp"),
        P("ep", "tp", None),
    )
    return jax.shard_map(
        body,
        mesh=mesh,
        in_specs=placed,
        out_specs=(P("ep", "tp"), P("ep", "tp", None, None), P("ep", "tp", None), P("ep", "tp")),
        check_vma=False,
    )
```

```python
import functools

import jax
import jax.numpy as jnp
from jax import lax
from jax.experimental import pallas as pl
from jax.experimental.pallas import tpu as pltpu
from jax.sharding import PartitionSpec as P


norm_epsilon = 1e-06


def room(mebibytes):
    return pltpu.CompilerParams(vmem_limit_bytes=mebibytes << 20)


def load_kernel(_, *refs, count, narrowed):
    sources, targets = refs[:count], refs[count : 2 * count]
    semaphores, *wide = refs[2 * count :]
    landed = wide + list(targets[narrowed:])
    copies = [
        pltpu.make_async_copy(source, target, semaphores.at[place])
        for place, (source, target) in enumerate(zip(sources, landed))
    ]
    for copy in copies:
        copy.start()
    for place, copy in enumerate(copies):
        copy.wait()
        if place < narrowed:

            @pl.loop(0, targets[place].shape[0])
            def narrow(row, place=place):
                targets[place][row] = wide[place][row].astype(jnp.bfloat16)


def load(after, arrays, narrowed=0):
    anywhere = pl.BlockSpec(memory_space=pl.ANY)
    targets = [
        pltpu.VMEM(array.shape, jnp.bfloat16 if place < narrowed else array.dtype)
        for place, array in enumerate(arrays)
    ]
    return pl.pallas_call(
        functools.partial(load_kernel, count=len(arrays), narrowed=narrowed),
        in_specs=[anywhere] * (len(arrays) + 1),
        out_specs=[pl.BlockSpec(memory_space=pltpu.VMEM)] * len(arrays),
        out_shape=targets,
        scratch_shapes=[pltpu.SemaphoreType.DMA((len(arrays),))]
        + [pltpu.VMEM(array.shape, array.dtype) for array in arrays[:narrowed]],
        compiler_params=room(12),
        cost_estimate=pl.CostEstimate(flops=1 << 22, bytes_accessed=0, transcendentals=0),
        name="load",
    )(after, *map(away, arrays))


def away(array):
    return pltpu.with_memory_space_constraint(array, pltpu.HBM)


def held(array):
    return pltpu.with_memory_space_constraint(array, pltpu.VMEM)


def pack_kernel(*refs):
    *sources, target, semaphores = refs
    copies = [
        pltpu.make_async_copy(source, target.at[place], semaphores.at[place])
        for place, source in enumerate(sources)
    ]
    for copy in copies:
        copy.start()
    for copy in copies:
        copy.wait()


def pack(weights):
    return pl.pallas_call(
        pack_kernel,
        in_specs=[pl.BlockSpec(memory_space=pl.ANY)] * len(weights),
        out_specs=pl.BlockSpec(memory_space=pltpu.VMEM),
        out_shape=pltpu.VMEM((len(weights),) + weights[0].shape, weights[0].dtype),
        scratch_shapes=[pltpu.SemaphoreType.DMA((len(weights),))],
        compiler_params=room(12),
        name="pack",
    )(*map(away, weights))


def split_kernel(rows_hbm, gain_hbm, out_ref, rows_ref, gain_ref, semaphores):
    copies = [
        pltpu.make_async_copy(rows_hbm, rows_ref, semaphores.at[0]),
        pltpu.make_async_copy(gain_hbm, gain_ref, semaphores.at[1]),
    ]
    for copy in copies:
        copy.start()
    for copy in copies:
        copy.wait()
    scaled = rows_ref[...].astype(jnp.float32) * gain_ref[...].astype(jnp.float32).reshape(1, -1)
    scaled = scaled.astype(jnp.bfloat16)
    seqs = rows_ref.shape[0]
    width = out_ref.shape[1]
    for place in range(out_ref.shape[0] // seqs):
        out_ref[place * seqs : (place + 1) * seqs, :] = scaled[:, place * width : (place + 1) * width]


def split_features(rows, gain, count):
    seqs, features = rows.shape
    width = features // count
    if width % 128:
        scaled = (rows.astype(jnp.float32) * gain.astype(jnp.float32)).astype(jnp.bfloat16)
        return scaled.reshape(seqs, count, width).transpose(1, 0, 2).reshape(count * seqs, width)
    return pl.pallas_call(
        split_kernel,
        in_specs=[pl.BlockSpec(memory_space=pl.ANY)] * 2,
        out_shape=jax.ShapeDtypeStruct((count * seqs, width), jnp.bfloat16),
        scratch_shapes=[
            pltpu.VMEM(rows.shape, rows.dtype),
            pltpu.VMEM(gain.shape, gain.dtype),
            pltpu.SemaphoreType.DMA((2,)),
        ],
        compiler_params=room(12),
        name="split_features",
    )(away(rows), away(gain))


def gates_kernel(
    index_ref,
    _,
    rows_ref,
    gain_ref,
    in_ref,
    forget_ref,
    bias_in_ref,
    bias_forget_ref,
    stab_ref,
    factor_ref,
    carry_ref,
    inflow_ref,
    stab_out_ref,
    in_pre_ref,
    forget_pre_ref,
):
    wide = rows_ref[...].astype(jnp.float32)
    factor = lax.rsqrt(jnp.mean(wide * wide, axis=-1, keepdims=True) + norm_epsilon)
    factor_ref[...] = factor
    normed = (wide * factor * gain_ref[...].astype(jnp.float32).reshape(1, -1)).astype(jnp.bfloat16)
    across = (((1,), (1,)), ((), ()))
    in_pre_ref[...] = lax.dot_general(in_ref[...], normed, across, preferred_element_type=jnp.float32)
    forget_pre_ref[...] = lax.dot_general(forget_ref[...], normed, across, preferred_element_type=jnp.float32)
    heads = stab_ref.shape[0]
    for head in range(heads):
        place = index_ref[0] * heads + head
        in_pre = in_pre_ref[pl.ds(place, 1), :] + bias_in_ref[place]
        forget_pre = forget_pre_ref[pl.ds(place, 1), :] + bias_forget_ref[place]
        log_forget = jnp.minimum(forget_pre, 0.0) - jnp.log1p(jnp.exp(-jnp.abs(forget_pre)))
        kept = log_forget + stab_ref[head : head + 1, :]
        stab_new = jnp.maximum(kept, in_pre)
        stab_out_ref[head : head + 1, :] = stab_new
        carry_ref[head : head + 1, :] = jnp.exp(kept - stab_new)
        inflow_ref[head : head + 1, :] = jnp.exp(in_pre - stab_new)


def gates(after, index, rows, gain, w_in, w_forget, bias_in, bias_forget, stab):
    seqs, heads = stab.shape
    small = jax.ShapeDtypeStruct((heads, seqs), jnp.float32)
    smem = pl.BlockSpec(memory_space=pltpu.SMEM)
    every = (w_in.shape[1], seqs)
    return pl.pallas_call(
        gates_kernel,
        in_specs=[smem, pl.BlockSpec(memory_space=pl.ANY)]
        + [pl.BlockSpec()] * 4
        + [smem] * 2
        + [pl.BlockSpec()],
        out_shape=[jax.ShapeDtypeStruct((seqs, 1), jnp.float32)] + [small] * 3,
        scratch_shapes=[pltpu.VMEM(every, jnp.float32)] * 2,
        compiler_params=room(12),
        cost_estimate=pl.CostEstimate(flops=1 << 22, bytes_accessed=0, transcendentals=0),
        name="gates",
    )(index, after, rows, gain, w_in.T, w_forget.T, bias_in, bias_forget, stab.T)


def project_kernel(index_ref, rows_ref, own_ref, other_ref, out_ref):
    count, features, width = own_ref.shape
    own = pl.multiple_of(index_ref[1] * features, features)
    other = pl.multiple_of((1 - index_ref[1]) * features, features)
    for place in range(count):
        total = jnp.dot(rows_ref[:, pl.ds(own, features)], own_ref[place], preferred_element_type=jnp.float32)
        total = total + jnp.dot(
            rows_ref[:, pl.ds(other, features)], other_ref[place], preferred_element_type=jnp.float32
        )
        out_ref[:, place * width : (place + 1) * width] = total.astype(jnp.bfloat16)


def project(index, rows, own, other):
    count, features, width = own.shape
    if features % 128:
        halves = rows.reshape(rows.shape[0], 2, -1)
        first = jnp.where(index[1] == 0, halves[:, 0], halves[:, 1])
        second = jnp.where(index[1] == 0, halves[:, 1], halves[:, 0])
        total = jnp.einsum("rf,cfw->rcw", first, own, preferred_element_type=jnp.float32)
        total = total + jnp.einsum("rf,cfw->rcw", second, other, preferred_element_type=jnp.float32)
        return total.astype(jnp.bfloat16).reshape(rows.shape[0], count * width)
    return pl.pallas_call(
        project_kernel,
        in_specs=[pl.BlockSpec(memory_space=pltpu.SMEM)] + [pl.BlockSpec()] * 3,
        out_shape=jax.ShapeDtypeStruct((rows.shape[0], count * width), jnp.bfloat16),
        compiler_params=room(12),
        name="project",
    )(index, rows, held(own), held(other))


def cell_kernel(
    index_ref,
    arrived_ref,
    factor_ref,
    carry_ref,
    inflow_ref,
    matrix_ref,
    normal_ref,
    proj_hbm,
    *refs,
    peers,
):
    term_refs = refs[:peers]
    rows_ref, proj_ref, semaphore = refs[peers:]
    proj_copy = pltpu.make_async_copy(proj_hbm, proj_ref, semaphore)
    proj_copy.start()
    seqs, heads, head_dim = matrix_ref.shape[:3]
    head_cols = heads * head_dim
    summed = jnp.sum(arrived_ref[...].astype(jnp.float32), axis=0) * factor_ref[...]
    summed = summed.astype(jnp.bfloat16).astype(jnp.float32)
    queries = jnp.concatenate(
        [
            jnp.concatenate(
                [
                    summed[:, head * head_dim : (head + 1) * head_dim]
                    if place == head
                    else jnp.zeros((seqs, head_dim), jnp.float32)
                    for place in range(heads)
                ],
                axis=1,
            )
            for head in range(heads)
        ],
        axis=0,
    ).astype(jnp.bfloat16)
    owner = lax.broadcasted_iota(jnp.int32, (heads * seqs, head_dim), 0) % seqs
    reads = jnp.zeros((heads * seqs, head_dim), jnp.float32)
    for seq in range(seqs):
        product = jnp.dot(
            queries, matrix_ref[seq].reshape(heads * head_dim, head_dim), preferred_element_type=jnp.float32
        )
        reads = jnp.where(owner == seq, product, reads)
    cells = []
    carries = carry_ref[...].T
    inflows = inflow_ref[...].T
    for head in range(heads):
        query, key, value, gate = [
            summed[:, start + head * head_dim : start + (head + 1) * head_dim]
            for start in range(0, 4 * head_cols, head_cols)
        ]
        carry = carries[:, head : head + 1]
        inflow = inflows[:, head : head + 1]
        inflow_key = inflow * (key * head_dim ** (-0.5))
        normal_new = carry * normal_ref[:, head, :] + inflow_key
        rows = slice(head * seqs, (head + 1) * seqs)
        rows_ref[0, rows, :] = key
        rows_ref[1, rows, :] = value
        rows_ref[2, rows, :] = jnp.broadcast_to(carry, (seqs, head_dim))
        rows_ref[3, rows, :] = jnp.broadcast_to(inflow * head_dim ** (-0.5), (seqs, head_dim))
        numer = carry * reads[rows] + jnp.sum(query * inflow_key, axis=-1, keepdims=True) * value
        denom = jnp.maximum(jnp.abs(jnp.sum(query * normal_new, axis=-1, keepdims=True)), 1.0)
        cells.append((numer / denom * jax.nn.sigmoid(gate)).astype(jnp.bfloat16))
    cell = jnp.concatenate(cells, axis=1)
    proj_copy.wait()
    width = proj_ref.shape[1] // peers
    for peer, term_ref in enumerate(term_refs):
        start = pl.multiple_of((index_ref[0] ^ peer) * width, width)
        term_ref[...] = jnp.dot(
            cell, proj_ref[:, pl.ds(start, width)], preferred_element_type=jnp.float32
        ).astype(jnp.bfloat16)


def cell_step(index, arrived, factor, carry, inflow, matrix_state, normal_rows, w_proj, peers):
    seqs, heads, head_dim, _ = matrix_state.shape
    wide = jnp.float32
    term = jax.ShapeDtypeStruct((seqs, w_proj.shape[1] // peers), jnp.bfloat16)
    by_head = jax.ShapeDtypeStruct((4, heads * seqs, head_dim), wide)
    vmem = pl.BlockSpec()
    return pl.pallas_call(
        functools.partial(cell_kernel, peers=peers),
        in_specs=[pl.BlockSpec(memory_space=pltpu.SMEM)]
        + [vmem] * 6
        + [pl.BlockSpec(memory_space=pl.ANY)],
        out_specs=[vmem] * (peers + 1),
        out_shape=[term] * peers
        + [by_head],
        scratch_shapes=[
            pltpu.VMEM(w_proj.shape, w_proj.dtype),
            pltpu.SemaphoreType.DMA,
        ],
        compiler_params=room(12),
        name="cell_step",
    )(index, held(arrived), factor, carry, inflow, held(matrix_state), normal_rows, away(w_proj))


def update_kernel(
    rows_ref,
    normal_ref,
    matrix_hbm,
    normal_out_ref,
    out_hbm,
    work_ref,
    loads,
    stores,
):
    seqs, heads, head_dim, _ = matrix_hbm.shape
    block = min(8, seqs)
    wide = (block, block * head_dim)
    own = lax.broadcasted_iota(jnp.int32, wide, 0) == lax.broadcasted_iota(jnp.int32, wide, 1) // head_dim

    def copy(step, out):
        part = pl.ds(step * block, block)
        if out:
            return pltpu.make_async_copy(work_ref.at[part], out_hbm.at[part], stores.at[step])
        return pltpu.make_async_copy(matrix_hbm.at[part], work_ref.at[part], loads.at[step])

    for step in range(seqs // block):
        copy(step, False).start()
    for head in range(heads):
        rows = slice(head * seqs, (head + 1) * seqs)
        normal_out_ref[:, head, :] = (
            rows_ref[2, rows, :] * normal_ref[:, head, :] + rows_ref[3, rows, :] * rows_ref[0, rows, :]
        )
    for step in range(seqs // block):
        copy(step, False).wait()
        for head in range(heads):
            rows = pl.ds(head * seqs + step * block, block)
            spread = jnp.where(own, jnp.concatenate([rows_ref[1, rows, :]] * block, axis=1), 0.0)
            outer = jnp.dot(
                rows_ref[0, rows, :].T.astype(jnp.bfloat16),
                spread.astype(jnp.bfloat16),
                preferred_element_type=jnp.float32,
            )
            for place in range(block):
                row = head * seqs + step * block + place
                seq = step * block + place
                work_ref[seq, head] = (
                    rows_ref[2, row : row + 1, :] * work_ref[seq, head]
                    + rows_ref[3, row : row + 1, :] * outer[:, place * head_dim : (place + 1) * head_dim]
                )
        copy(step, True).start()
    for step in range(seqs // block):
        copy(step, True).wait()


def update_states(rows, normal_state, matrix_state):
    anywhere = pl.BlockSpec(memory_space=pl.ANY)
    steps = matrix_state.shape[0] // min(8, matrix_state.shape[0])
    return pl.pallas_call(
        update_kernel,
        in_specs=[pl.BlockSpec()] * 2 + [anywhere],
        out_specs=[pl.BlockSpec(), anywhere],
        out_shape=[
            jax.ShapeDtypeStruct(normal_state.shape, jnp.float32),
            pltpu.HBM(matrix_state.shape, jnp.float32),
        ],
        scratch_shapes=[
            pltpu.VMEM(matrix_state.shape, jnp.float32),
            pltpu.SemaphoreType.DMA((steps,)),
            pltpu.SemaphoreType.DMA((steps,)),
        ],
        compiler_params=room(12),
        cost_estimate=pl.CostEstimate(flops=1 << 23, bytes_accessed=0, transcendentals=0),
        name="update_states",
    )(rows, normal_state, away(matrix_state))


def expert_kernel(index_ref, *refs, peers, halves):
    count = peers * halves
    chunk_refs = refs[:count]
    gain_ref, gate_ref, up_ref, down_ref = refs[count : count + 4]
    term_refs = refs[count + 4 :]
    _, width = chunk_refs[0].shape
    squares = [
        sum(
            jnp.sum(jnp.square(chunk_refs[half * peers + peer][...].astype(jnp.float32)), axis=-1, keepdims=True)
            for peer in range(peers)
        )
        for half in range(halves)
    ]
    factors = [lax.rsqrt(square / (peers * width) + norm_epsilon) for square in squares]
    for half in range(halves):
        gate_sum = up_sum = None
        for peer in range(peers):
            columns = pl.ds(pl.multiple_of((index_ref[0] ^ peer) * width, width), width)
            gain = gain_ref[:, columns].astype(jnp.float32)
            chunk = chunk_refs[half * peers + peer][...].astype(jnp.float32)
            normed = (chunk * factors[half] * gain).astype(jnp.bfloat16)
            gate_part = jnp.dot(normed, gate_ref[0, columns, :], preferred_element_type=jnp.float32)
            up_part = jnp.dot(normed, up_ref[0, columns, :], preferred_element_type=jnp.float32)
            gate_sum = gate_part if peer == 0 else gate_sum + gate_part
            up_sum = up_part if peer == 0 else up_sum + up_part
        inner = (jax.nn.silu(gate_sum) * up_sum).astype(jnp.bfloat16)
        for peer in range(peers):
            columns = pl.ds(pl.multiple_of((index_ref[0] ^ peer) * width, width), width)
            term_refs[half * peers + peer][...] = jnp.dot(
                inner, down_ref[0, :, columns], preferred_element_type=jnp.float32
            ).astype(jnp.bfloat16)


def expert_step(index, chunks, gain, gate, up, down, peers):
    vmem = pl.BlockSpec()
    return pl.pallas_call(
        functools.partial(expert_kernel, peers=peers, halves=len(chunks) // peers),
        in_specs=[pl.BlockSpec(memory_space=pltpu.SMEM)]
        + [vmem] * (len(chunks) + 4),
        out_specs=[vmem] * len(chunks),
        out_shape=[jax.ShapeDtypeStruct(chunks[0].shape, jnp.bfloat16)] * len(chunks),
        compiler_params=room(12),
        name="expert_step",
    )(index, *map(held, chunks), gain, held(gate), held(up), held(down))


def dispatch_table(route_ids, experts, capacity):
    flat_ids = route_ids.reshape(-1)
    expert_hot = (flat_ids[:, None] == jnp.arange(experts, dtype=jnp.int32)[None, :]).astype(
        jnp.int32
    )
    slot_rank = jnp.sum((jnp.cumsum(expert_hot, axis=0) - 1) * expert_hot, axis=1)
    slot_hot = (slot_rank[:, None] == jnp.arange(capacity, dtype=jnp.int32)[None, :]).astype(
        jnp.float32
    )
    table = expert_hot.astype(jnp.float32)[:, :, None] * slot_hot[:, None, :]
    return table.reshape(flat_ids.shape[0], experts * capacity)


def pack_rows(table, row_block, top_count, experts, capacity):
    repeated = jnp.repeat(row_block, top_count, axis=0)
    packed = jnp.einsum(
        "as,aw->sw", table.astype(jnp.bfloat16), repeated, preferred_element_type=jnp.float32
    ).astype(jnp.bfloat16)
    return packed.reshape(experts, capacity, row_block.shape[1])


def swap(value, half, peer):
    ep_count, tp_count = lax.axis_size("ep"), lax.axis_size("tp")
    away = half * tp_count + peer
    return lax.ppermute(value, ("ep", "tp"), [(i, i ^ away) for i in range(ep_count * tp_count)])


def far_places(peers):
    return [(half, peer) for half in range(2) for peer in range(0, peers, 2)]


def gather_chunks(own, peers, beside):
    chunks = {}
    for half, peer in far_places(peers):
        chunks[half, peer] = swap(own, half, peer) if half or peer else own
    first = (0, 2) if peers > 2 else (1, 0)
    chunks[first], beside = lax.optimization_barrier((chunks[first], beside))
    for half, peer in far_places(peers):
        chunks[half, peer ^ 1] = swap(chunks[half, peer], 0, 1)
    return [chunks[half, peer] for half in range(2) for peer in range(peers)], beside


def sum_chunks(terms, peers):
    left = {(place // peers, place % peers): term for place, term in enumerate(terms)}
    places = far_places(peers)
    for half, peer in places[1:] + places[:1]:
        other = swap(left[half, peer ^ 1], 0, 1)
        left[half, peer] = left[half, peer].astype(jnp.float32) + other.astype(jnp.float32)
    total = left[0, 0]
    for half, peer in places[1:]:
        total = total + swap(left[half, peer].astype(jnp.bfloat16), half, peer).astype(jnp.float32)
    return total


def body(
    tokens,
    gain_mix,
    gain_ffn,
    w_query,
    w_key,
    w_value,
    w_outgate,
    w_ingate,
    w_forget,
    bias_in,
    bias_forget,
    w_proj,
    matrix_state,
    normal_state,
    stab_state,
    route_ids,
    route_weights,
    w_exp_gate,
    w_exp_up,
    w_exp_down,
):
    ep_count = lax.axis_size("ep")
    tp_count = lax.axis_size("tp")
    tp_index = lax.axis_index("tp")
    seq_dev = tokens.shape[0]
    model_width = tokens.shape[1]
    head_cols = w_query.shape[1]
    top_count = route_ids.shape[1]
    experts = ep_count // 2
    capacity = min(seq_dev, max(2, 2 * seq_dev * top_count // experts))
    every_row = capacity == seq_dev
    col_width = model_width // tp_count
    index = jnp.stack([tp_index, lax.axis_index("ep") % 2]).astype(jnp.int32)
    own_weights = pack((w_query, w_key, w_value, w_outgate))
    other_weights = swap(own_weights, 1, 0)
    blocks = split_features(tokens, gain_mix, experts)
    same_half = [list(range(half, ep_count, 2)) for half in range(2)]

    def exchange(rows):
        return lax.all_to_all(
            rows, "ep", split_axis=0, concat_axis=0, tiled=True, axis_index_groups=same_half
        )

    blocks, index = lax.optimization_barrier((blocks, index))
    foreign = exchange(blocks)
    terms = project(index, foreign, own_weights, other_weights)
    (held_state,) = load(terms, (matrix_state,), narrowed=1)
    arrived = exchange(terms)
    factor, carry, inflow, stab_turned = gates(
        terms, index, tokens, gain_mix, w_ingate, w_forget, bias_in, bias_forget, stab_state
    )
    stab_new = stab_turned.T
    weights = route_weights / jnp.sum(route_weights, axis=-1, keepdims=True)
    if every_row:
        chosen = route_ids[:, :, None] == jnp.arange(experts, dtype=jnp.int32)
        shares = jnp.sum(jnp.where(chosen, weights[:, :, None], 0.0), axis=1)
    else:
        shares = weights
    factor, shares, stab_new = lax.optimization_barrier((factor, shares, stab_new))
    cell_outs = cell_step(
        index,
        arrived.reshape(experts, seq_dev, 4 * head_cols),
        factor,
        carry,
        inflow,
        held_state,
        normal_state,
        w_proj,
        tp_count,
    )
    *out_terms, state_rows = cell_outs
    normal_new, matrix_new = update_states(state_rows, normal_state, matrix_state)
    own_tokens = lax.dynamic_slice_in_dim(tokens, tp_index * col_width, col_width, 1)
    attended = out_terms[0].astype(jnp.float32)
    for peer in range(1, tp_count):
        attended = attended + swap(out_terms[peer], 0, peer).astype(jnp.float32)
    own_resid = (own_tokens.astype(jnp.float32) + attended).astype(jnp.bfloat16)
    held_experts = load(held(state_rows), (w_exp_gate, w_exp_up))
    own_resid, *held_experts = lax.optimization_barrier((own_resid, *held_experts))
    if every_row:
        packed = jnp.broadcast_to(own_resid, (experts, seq_dev, col_width))
    else:
        table = dispatch_table(route_ids, experts, capacity)
        packed = pack_rows(table, own_resid, top_count, experts, capacity)
    received = exchange(packed.reshape(experts * capacity, col_width))
    (held_down,) = load(received, (w_exp_down,))
    chunks, held_down = gather_chunks(received, tp_count, held_down)
    down_terms = expert_step(
        index,
        chunks,
        gain_ffn.reshape(1, model_width),
        *held_experts,
        held_down,
        tp_count,
    )
    half_share = sum_chunks(down_terms, tp_count).astype(jnp.bfloat16)
    half_share, matrix_new, normal_new = lax.optimization_barrier((half_share, matrix_new, normal_new))
    returned = exchange(half_share).astype(jnp.float32).reshape(experts, capacity, col_width)
    if every_row:
        routed = jnp.sum(returned * shares.T[:, :, None], axis=0)
    else:
        combine = jnp.sum(
            (table * shares.reshape(-1)[:, None]).reshape(
                seq_dev, top_count, experts * capacity
            ),
            axis=1,
        )
        routed = jnp.dot(
            combine, returned.reshape(experts * capacity, col_width), precision=lax.Precision.HIGHEST
        )
    mixed_out = (own_resid.astype(jnp.float32) + routed).astype(jnp.bfloat16)
    return (mixed_out, matrix_new, normal_new, stab_new)


def solution(mesh):
    placed = (
        P("ep", None),
        P(),
        P(),
        P("ep", "tp"),
        P("ep", "tp"),
        P("ep", "tp"),
        P("ep", "tp"),
        P(),
        P(),
        P(),
        P(),
        P("tp", None),
        P("ep", "tp", None, None),
        P("ep", "tp", None),
        P("ep", "tp"),
        P("ep", None),
        P("ep", None),
        P("ep", None, "tp"),
        P("ep", None, "tp"),
        P("ep", "tp", None),
    )
    return jax.shard_map(
        body,
        mesh=mesh,
        in_specs=placed,
        out_specs=(P("ep", "tp"), P("ep", "tp", None, None), P("ep", "tp", None), P("ep", "tp")),
        check_vma=False,
    )
```

```python
import functools

import jax
import jax.numpy as jnp
from jax import lax
from jax.experimental import pallas as pl
from jax.experimental.pallas import tpu as pltpu
from jax.sharding import PartitionSpec as P


norm_epsilon = 1e-06


def room(mebibytes):
    return pltpu.CompilerParams(vmem_limit_bytes=mebibytes << 20)


def load_kernel(_, *refs, count, narrowed):
    sources, targets = refs[:count], refs[count : 2 * count]
    semaphores, *wide = refs[2 * count :]
    landed = wide + list(targets[narrowed:])
    copies = [
        pltpu.make_async_copy(source, target, semaphores.at[place])
        for place, (source, target) in enumerate(zip(sources, landed))
    ]
    for copy in copies:
        copy.start()
    for place, copy in enumerate(copies):
        copy.wait()
        if place < narrowed:

            @pl.loop(0, targets[place].shape[0])
            def narrow(row, place=place):
                targets[place][row] = wide[place][row].astype(jnp.bfloat16)


def load(after, arrays, narrowed=0):
    anywhere = pl.BlockSpec(memory_space=pl.ANY)
    targets = [
        pltpu.VMEM(array.shape, jnp.bfloat16 if place < narrowed else array.dtype)
        for place, array in enumerate(arrays)
    ]
    return pl.pallas_call(
        functools.partial(load_kernel, count=len(arrays), narrowed=narrowed),
        in_specs=[anywhere] * (len(arrays) + 1),
        out_specs=[pl.BlockSpec(memory_space=pltpu.VMEM)] * len(arrays),
        out_shape=targets,
        scratch_shapes=[pltpu.SemaphoreType.DMA((len(arrays),))]
        + [pltpu.VMEM(array.shape, array.dtype) for array in arrays[:narrowed]],
        compiler_params=room(12),
        cost_estimate=pl.CostEstimate(flops=1 << 22, bytes_accessed=0, transcendentals=0),
        name="load",
    )(after, *map(away, arrays))


def away(array):
    return pltpu.with_memory_space_constraint(array, pltpu.HBM)


def held(array):
    return pltpu.with_memory_space_constraint(array, pltpu.VMEM)


def pack_kernel(*refs):
    *sources, target, semaphores = refs
    copies = [
        pltpu.make_async_copy(source, target.at[place], semaphores.at[place])
        for place, source in enumerate(sources)
    ]
    for copy in copies:
        copy.start()
    for copy in copies:
        copy.wait()


def pack(weights):
    return pl.pallas_call(
        pack_kernel,
        in_specs=[pl.BlockSpec(memory_space=pl.ANY)] * len(weights),
        out_specs=pl.BlockSpec(memory_space=pltpu.VMEM),
        out_shape=pltpu.VMEM((len(weights),) + weights[0].shape, weights[0].dtype),
        scratch_shapes=[pltpu.SemaphoreType.DMA((len(weights),))],
        compiler_params=room(12),
        name="pack",
    )(*map(away, weights))


def split_kernel(rows_hbm, gain_hbm, out_ref, rows_ref, gain_ref, semaphores):
    copies = [
        pltpu.make_async_copy(rows_hbm, rows_ref, semaphores.at[0]),
        pltpu.make_async_copy(gain_hbm, gain_ref, semaphores.at[1]),
    ]
    for copy in copies:
        copy.start()
    for copy in copies:
        copy.wait()
    scaled = rows_ref[...].astype(jnp.float32) * gain_ref[...].astype(jnp.float32).reshape(1, -1)
    scaled = scaled.astype(jnp.bfloat16)
    seqs = rows_ref.shape[0]
    width = out_ref.shape[1]
    for place in range(out_ref.shape[0] // seqs):
        out_ref[place * seqs : (place + 1) * seqs, :] = scaled[:, place * width : (place + 1) * width]


def split_features(rows, gain, count):
    seqs, features = rows.shape
    width = features // count
    if width % 128:
        scaled = (rows.astype(jnp.float32) * gain.astype(jnp.float32)).astype(jnp.bfloat16)
        return scaled.reshape(seqs, count, width).transpose(1, 0, 2).reshape(count * seqs, width)
    return pl.pallas_call(
        split_kernel,
        in_specs=[pl.BlockSpec(memory_space=pl.ANY)] * 2,
        out_shape=jax.ShapeDtypeStruct((count * seqs, width), jnp.bfloat16),
        scratch_shapes=[
            pltpu.VMEM(rows.shape, rows.dtype),
            pltpu.VMEM(gain.shape, gain.dtype),
            pltpu.SemaphoreType.DMA((2,)),
        ],
        compiler_params=room(12),
        name="split_features",
    )(away(rows), away(gain))


def gates_kernel(
    index_ref,
    _,
    rows_ref,
    gain_ref,
    in_ref,
    forget_ref,
    bias_in_ref,
    bias_forget_ref,
    stab_ref,
    factor_ref,
    carry_ref,
    inflow_ref,
    stab_out_ref,
    in_pre_ref,
    forget_pre_ref,
):
    wide = rows_ref[...].astype(jnp.float32)
    factor = lax.rsqrt(jnp.mean(wide * wide, axis=-1, keepdims=True) + norm_epsilon)
    factor_ref[...] = factor
    normed = (wide * factor * gain_ref[...].astype(jnp.float32).reshape(1, -1)).astype(jnp.bfloat16)
    across = (((1,), (1,)), ((), ()))
    in_pre_ref[...] = lax.dot_general(in_ref[...], normed, across, preferred_element_type=jnp.float32)
    forget_pre_ref[...] = lax.dot_general(forget_ref[...], normed, across, preferred_element_type=jnp.float32)
    heads = stab_ref.shape[0]
    for head in range(heads):
        place = index_ref[0] * heads + head
        in_pre = in_pre_ref[pl.ds(place, 1), :] + bias_in_ref[place]
        forget_pre = forget_pre_ref[pl.ds(place, 1), :] + bias_forget_ref[place]
        log_forget = jnp.minimum(forget_pre, 0.0) - jnp.log1p(jnp.exp(-jnp.abs(forget_pre)))
        kept = log_forget + stab_ref[head : head + 1, :]
        stab_new = jnp.maximum(kept, in_pre)
        stab_out_ref[head : head + 1, :] = stab_new
        carry_ref[head : head + 1, :] = jnp.exp(kept - stab_new)
        inflow_ref[head : head + 1, :] = jnp.exp(in_pre - stab_new)


def gates(after, index, rows, gain, w_in, w_forget, bias_in, bias_forget, stab):
    seqs, heads = stab.shape
    small = jax.ShapeDtypeStruct((heads, seqs), jnp.float32)
    smem = pl.BlockSpec(memory_space=pltpu.SMEM)
    every = (w_in.shape[1], seqs)
    return pl.pallas_call(
        gates_kernel,
        in_specs=[smem, pl.BlockSpec(memory_space=pl.ANY)]
        + [pl.BlockSpec()] * 4
        + [smem] * 2
        + [pl.BlockSpec()],
        out_shape=[jax.ShapeDtypeStruct((seqs, 1), jnp.float32)] + [small] * 3,
        scratch_shapes=[pltpu.VMEM(every, jnp.float32)] * 2,
        compiler_params=room(12),
        cost_estimate=pl.CostEstimate(flops=1 << 22, bytes_accessed=0, transcendentals=0),
        name="gates",
    )(index, after, rows, gain, w_in.T, w_forget.T, bias_in, bias_forget, stab.T)


def project_kernel(index_ref, rows_ref, own_ref, other_ref, out_ref):
    count, features, width = own_ref.shape
    own = pl.multiple_of(index_ref[1] * features, features)
    other = pl.multiple_of((1 - index_ref[1]) * features, features)
    for place in range(count):
        total = jnp.dot(rows_ref[:, pl.ds(own, features)], own_ref[place], preferred_element_type=jnp.float32)
        total = total + jnp.dot(
            rows_ref[:, pl.ds(other, features)], other_ref[place], preferred_element_type=jnp.float32
        )
        out_ref[:, place * width : (place + 1) * width] = total.astype(jnp.bfloat16)


def project(index, rows, own, other):
    count, features, width = own.shape
    if features % 128:
        halves = rows.reshape(rows.shape[0], 2, -1)
        first = jnp.where(index[1] == 0, halves[:, 0], halves[:, 1])
        second = jnp.where(index[1] == 0, halves[:, 1], halves[:, 0])
        total = jnp.einsum("rf,cfw->rcw", first, own, preferred_element_type=jnp.float32)
        total = total + jnp.einsum("rf,cfw->rcw", second, other, preferred_element_type=jnp.float32)
        return total.astype(jnp.bfloat16).reshape(rows.shape[0], count * width)
    return pl.pallas_call(
        project_kernel,
        in_specs=[pl.BlockSpec(memory_space=pltpu.SMEM)] + [pl.BlockSpec()] * 3,
        out_shape=jax.ShapeDtypeStruct((rows.shape[0], count * width), jnp.bfloat16),
        compiler_params=room(12),
        name="project",
    )(index, rows, held(own), held(other))


def cell_kernel(
    index_ref,
    arrived_ref,
    factor_ref,
    carry_ref,
    inflow_ref,
    matrix_ref,
    normal_ref,
    proj_hbm,
    *refs,
    peers,
):
    term_refs = refs[:peers]
    rows_ref, proj_ref, semaphore = refs[peers:]
    proj_copy = pltpu.make_async_copy(proj_hbm, proj_ref, semaphore)
    proj_copy.start()
    seqs, heads, head_dim = matrix_ref.shape[:3]
    head_cols = heads * head_dim
    summed = jnp.sum(arrived_ref[...].astype(jnp.float32), axis=0) * factor_ref[...]
    summed = summed.astype(jnp.bfloat16).astype(jnp.float32)
    queries = jnp.concatenate(
        [
            jnp.concatenate(
                [
                    summed[:, head * head_dim : (head + 1) * head_dim]
                    if place == head
                    else jnp.zeros((seqs, head_dim), jnp.float32)
                    for place in range(heads)
                ],
                axis=1,
            )
            for head in range(heads)
        ],
        axis=0,
    ).astype(jnp.bfloat16)
    owner = lax.broadcasted_iota(jnp.int32, (heads * seqs, head_dim), 0) % seqs
    reads = jnp.zeros((heads * seqs, head_dim), jnp.float32)
    for seq in range(seqs):
        product = jnp.dot(
            queries, matrix_ref[seq].reshape(heads * head_dim, head_dim), preferred_element_type=jnp.float32
        )
        reads = jnp.where(owner == seq, product, reads)
    cells = []
    carries = carry_ref[...].T
    inflows = inflow_ref[...].T
    for head in range(heads):
        query, key, value, gate = [
            summed[:, start + head * head_dim : start + (head + 1) * head_dim]
            for start in range(0, 4 * head_cols, head_cols)
        ]
        carry = carries[:, head : head + 1]
        inflow = inflows[:, head : head + 1]
        inflow_key = inflow * (key * head_dim ** (-0.5))
        normal_new = carry * normal_ref[:, head, :] + inflow_key
        rows = slice(head * seqs, (head + 1) * seqs)
        rows_ref[0, rows, :] = key
        rows_ref[1, rows, :] = value
        rows_ref[2, rows, :] = jnp.broadcast_to(carry, (seqs, head_dim))
        rows_ref[3, rows, :] = jnp.broadcast_to(inflow * head_dim ** (-0.5), (seqs, head_dim))
        numer = carry * reads[rows] + jnp.sum(query * inflow_key, axis=-1, keepdims=True) * value
        denom = jnp.maximum(jnp.abs(jnp.sum(query * normal_new, axis=-1, keepdims=True)), 1.0)
        cells.append((numer / denom * jax.nn.sigmoid(gate)).astype(jnp.bfloat16))
    cell = jnp.concatenate(cells, axis=1)
    proj_copy.wait()
    width = proj_ref.shape[1] // peers
    for peer, term_ref in enumerate(term_refs):
        start = pl.multiple_of((index_ref[0] ^ peer) * width, width)
        term_ref[...] = jnp.dot(
            cell, proj_ref[:, pl.ds(start, width)], preferred_element_type=jnp.float32
        ).astype(jnp.bfloat16)


def cell_step(index, arrived, factor, carry, inflow, matrix_state, normal_rows, w_proj, peers):
    seqs, heads, head_dim, _ = matrix_state.shape
    wide = jnp.float32
    term = jax.ShapeDtypeStruct((seqs, w_proj.shape[1] // peers), jnp.bfloat16)
    by_head = jax.ShapeDtypeStruct((4, heads * seqs, head_dim), wide)
    vmem = pl.BlockSpec()
    return pl.pallas_call(
        functools.partial(cell_kernel, peers=peers),
        in_specs=[pl.BlockSpec(memory_space=pltpu.SMEM)]
        + [vmem] * 6
        + [pl.BlockSpec(memory_space=pl.ANY)],
        out_specs=[vmem] * (peers + 1),
        out_shape=[term] * peers
        + [by_head],
        scratch_shapes=[
            pltpu.VMEM(w_proj.shape, w_proj.dtype),
            pltpu.SemaphoreType.DMA,
        ],
        compiler_params=room(12),
        name="cell_step",
    )(index, held(arrived), factor, carry, inflow, held(matrix_state), normal_rows, away(w_proj))


def update_kernel(
    rows_ref,
    normal_ref,
    matrix_hbm,
    normal_out_ref,
    out_hbm,
    work_ref,
    loads,
    stores,
):
    seqs, heads, head_dim, _ = matrix_hbm.shape
    block = min(8, seqs)
    wide = (block, block * head_dim)
    own = lax.broadcasted_iota(jnp.int32, wide, 0) == lax.broadcasted_iota(jnp.int32, wide, 1) // head_dim

    def copy(step, out):
        part = pl.ds(step * block, block)
        if out:
            return pltpu.make_async_copy(work_ref.at[part], out_hbm.at[part], stores.at[step])
        return pltpu.make_async_copy(matrix_hbm.at[part], work_ref.at[part], loads.at[step])

    for step in range(seqs // block):
        copy(step, False).start()
    for head in range(heads):
        rows = slice(head * seqs, (head + 1) * seqs)
        normal_out_ref[:, head, :] = (
            rows_ref[2, rows, :] * normal_ref[:, head, :] + rows_ref[3, rows, :] * rows_ref[0, rows, :]
        )
    for step in range(seqs // block):
        copy(step, False).wait()
        for head in range(heads):
            rows = pl.ds(head * seqs + step * block, block)
            spread = jnp.where(own, jnp.concatenate([rows_ref[1, rows, :]] * block, axis=1), 0.0)
            outer = jnp.dot(
                rows_ref[0, rows, :].T.astype(jnp.bfloat16),
                spread.astype(jnp.bfloat16),
                preferred_element_type=jnp.float32,
            )
            for place in range(block):
                row = head * seqs + step * block + place
                seq = step * block + place
                work_ref[seq, head] = (
                    rows_ref[2, row : row + 1, :] * work_ref[seq, head]
                    + rows_ref[3, row : row + 1, :] * outer[:, place * head_dim : (place + 1) * head_dim]
                )
        copy(step, True).start()
    for step in range(seqs // block):
        copy(step, True).wait()


def update_states(rows, normal_state, matrix_state):
    anywhere = pl.BlockSpec(memory_space=pl.ANY)
    steps = matrix_state.shape[0] // min(8, matrix_state.shape[0])
    return pl.pallas_call(
        update_kernel,
        in_specs=[pl.BlockSpec()] * 2 + [anywhere],
        out_specs=[pl.BlockSpec(), anywhere],
        out_shape=[
            jax.ShapeDtypeStruct(normal_state.shape, jnp.float32),
            pltpu.HBM(matrix_state.shape, jnp.float32),
        ],
        scratch_shapes=[
            pltpu.VMEM(matrix_state.shape, jnp.float32),
            pltpu.SemaphoreType.DMA((steps,)),
            pltpu.SemaphoreType.DMA((steps,)),
        ],
        compiler_params=room(12),
        cost_estimate=pl.CostEstimate(flops=1 << 23, bytes_accessed=0, transcendentals=0),
        name="update_states",
    )(rows, normal_state, away(matrix_state))


def expert_kernel(index_ref, *refs, peers, halves):
    count = peers * halves
    chunk_refs = refs[:count]
    gain_ref, gate_ref, up_ref, down_ref = refs[count : count + 4]
    term_refs = refs[count + 4 :]
    _, width = chunk_refs[0].shape
    squares = [
        sum(
            jnp.sum(jnp.square(chunk_refs[half * peers + peer][...].astype(jnp.float32)), axis=-1, keepdims=True)
            for peer in range(peers)
        )
        for half in range(halves)
    ]
    factors = [lax.rsqrt(square / (peers * width) + norm_epsilon) for square in squares]
    for half in range(halves):
        gate_sum = up_sum = None
        for peer in range(peers):
            columns = pl.ds(pl.multiple_of((index_ref[0] ^ peer) * width, width), width)
            gain = gain_ref[:, columns].astype(jnp.float32)
            chunk = chunk_refs[half * peers + peer][...].astype(jnp.float32)
            normed = (chunk * factors[half] * gain).astype(jnp.bfloat16)
            gate_part = jnp.dot(normed, gate_ref[0, columns, :], preferred_element_type=jnp.float32)
            up_part = jnp.dot(normed, up_ref[0, columns, :], preferred_element_type=jnp.float32)
            gate_sum = gate_part if peer == 0 else gate_sum + gate_part
            up_sum = up_part if peer == 0 else up_sum + up_part
        inner = (jax.nn.silu(gate_sum) * up_sum).astype(jnp.bfloat16)
        for peer in range(peers):
            columns = pl.ds(pl.multiple_of((index_ref[0] ^ peer) * width, width), width)
            term_refs[half * peers + peer][...] = jnp.dot(
                inner, down_ref[0, :, columns], preferred_element_type=jnp.float32
            ).astype(jnp.bfloat16)


def expert_step(index, chunks, gain, gate, up, down, peers):
    vmem = pl.BlockSpec()
    return pl.pallas_call(
        functools.partial(expert_kernel, peers=peers, halves=len(chunks) // peers),
        in_specs=[pl.BlockSpec(memory_space=pltpu.SMEM)]
        + [vmem] * (len(chunks) + 4),
        out_specs=[vmem] * len(chunks),
        out_shape=[jax.ShapeDtypeStruct(chunks[0].shape, jnp.bfloat16)] * len(chunks),
        compiler_params=room(12),
        name="expert_step",
    )(index, *map(held, chunks), gain, held(gate), held(up), held(down))


def dispatch_table(route_ids, experts, capacity):
    flat_ids = route_ids.reshape(-1)
    expert_hot = (flat_ids[:, None] == jnp.arange(experts, dtype=jnp.int32)[None, :]).astype(
        jnp.int32
    )
    slot_rank = jnp.sum((jnp.cumsum(expert_hot, axis=0) - 1) * expert_hot, axis=1)
    slot_hot = (slot_rank[:, None] == jnp.arange(capacity, dtype=jnp.int32)[None, :]).astype(
        jnp.float32
    )
    table = expert_hot.astype(jnp.float32)[:, :, None] * slot_hot[:, None, :]
    return table.reshape(flat_ids.shape[0], experts * capacity)


def pack_rows(table, row_block, top_count, experts, capacity):
    repeated = jnp.repeat(row_block, top_count, axis=0)
    packed = jnp.einsum(
        "as,aw->sw", table.astype(jnp.bfloat16), repeated, preferred_element_type=jnp.float32
    ).astype(jnp.bfloat16)
    return packed.reshape(experts, capacity, row_block.shape[1])


def swap(value, half, peer):
    ep_count, tp_count = lax.axis_size("ep"), lax.axis_size("tp")
    away = half * tp_count + peer
    return lax.ppermute(value, ("ep", "tp"), [(i, i ^ away) for i in range(ep_count * tp_count)])


def far_places(peers):
    return [(half, peer) for half in range(2) for peer in range(0, peers, 2)]


def gather_chunks(own, peers, beside):
    chunks = {}
    for half, peer in far_places(peers):
        chunks[half, peer] = swap(own, half, peer) if half or peer else own
    first = (0, 2) if peers > 2 else (1, 0)
    chunks[first], beside = lax.optimization_barrier((chunks[first], beside))
    for half, peer in far_places(peers):
        chunks[half, peer ^ 1] = swap(chunks[half, peer], 0, 1)
    return [chunks[half, peer] for half in range(2) for peer in range(peers)], beside


def sum_chunks(terms, peers):
    left = {(place // peers, place % peers): term for place, term in enumerate(terms)}
    places = far_places(peers)
    for half, peer in places[1:] + places[:1]:
        other = swap(left[half, peer ^ 1], 0, 1)
        left[half, peer] = left[half, peer].astype(jnp.float32) + other.astype(jnp.float32)
    total = left[0, 0]
    for half, peer in places[1:]:
        other = swap(left[half, peer].astype(jnp.bfloat16), half, peer)
        total = total + other.astype(jnp.float32)
    return total


def body(
    tokens,
    gain_mix,
    gain_ffn,
    w_query,
    w_key,
    w_value,
    w_outgate,
    w_ingate,
    w_forget,
    bias_in,
    bias_forget,
    w_proj,
    matrix_state,
    normal_state,
    stab_state,
    route_ids,
    route_weights,
    w_exp_gate,
    w_exp_up,
    w_exp_down,
):
    ep_count = lax.axis_size("ep")
    tp_count = lax.axis_size("tp")
    tp_index = lax.axis_index("tp")
    seq_dev = tokens.shape[0]
    model_width = tokens.shape[1]
    head_cols = w_query.shape[1]
    top_count = route_ids.shape[1]
    experts = ep_count // 2
    capacity = min(seq_dev, max(2, 2 * seq_dev * top_count // experts))
    every_row = capacity == seq_dev
    col_width = model_width // tp_count
    index = jnp.stack([tp_index, lax.axis_index("ep") % 2]).astype(jnp.int32)
    own_weights = pack((w_query, w_key, w_value, w_outgate))
    other_weights = swap(own_weights, 1, 0)
    blocks = split_features(tokens, gain_mix, experts)
    same_half = [list(range(half, ep_count, 2)) for half in range(2)]

    def exchange(rows):
        return lax.all_to_all(
            rows, "ep", split_axis=0, concat_axis=0, tiled=True, axis_index_groups=same_half
        )

    blocks, index = lax.optimization_barrier((blocks, index))
    foreign = exchange(blocks)
    terms = project(index, foreign, own_weights, other_weights)
    (held_state,) = load(terms, (matrix_state,), narrowed=1)
    arrived = exchange(terms)
    factor, carry, inflow, stab_turned = gates(
        terms, index, tokens, gain_mix, w_ingate, w_forget, bias_in, bias_forget, stab_state
    )
    stab_new = stab_turned.T
    weights = route_weights / jnp.sum(route_weights, axis=-1, keepdims=True)
    if every_row:
        chosen = route_ids[:, :, None] == jnp.arange(experts, dtype=jnp.int32)
        shares = jnp.sum(jnp.where(chosen, weights[:, :, None], 0.0), axis=1)
    else:
        shares = weights
    factor, shares, stab_new = lax.optimization_barrier((factor, shares, stab_new))
    cell_outs = cell_step(
        index,
        arrived.reshape(experts, seq_dev, 4 * head_cols),
        factor,
        carry,
        inflow,
        held_state,
        normal_state,
        w_proj,
        tp_count,
    )
    *out_terms, state_rows = cell_outs
    normal_new, matrix_new = update_states(state_rows, normal_state, matrix_state)
    own_tokens = lax.dynamic_slice_in_dim(tokens, tp_index * col_width, col_width, 1)
    attended = out_terms[0].astype(jnp.float32)
    for peer in range(1, tp_count):
        attended = attended + swap(out_terms[peer], 0, peer).astype(jnp.float32)
    own_resid = (own_tokens.astype(jnp.float32) + attended).astype(jnp.bfloat16)
    held_experts = load(held(state_rows), (w_exp_gate, w_exp_up))
    own_resid, *held_experts = lax.optimization_barrier((own_resid, *held_experts))
    if every_row:
        packed = jnp.broadcast_to(own_resid, (experts, seq_dev, col_width))
    else:
        table = dispatch_table(route_ids, experts, capacity)
        packed = pack_rows(table, own_resid, top_count, experts, capacity)
    received = exchange(packed.reshape(experts * capacity, col_width))
    (held_down,) = load(received, (w_exp_down,))
    chunks, held_down = gather_chunks(received, tp_count, held_down)
    down_terms = []
    for half in range(2):
        down_terms += expert_step(
            index,
            chunks[half * tp_count : (half + 1) * tp_count],
            gain_ffn.reshape(1, model_width),
            *held_experts,
            held_down,
            tp_count,
        )
    half_share = sum_chunks(down_terms, tp_count).astype(jnp.bfloat16)
    half_share, matrix_new, normal_new = lax.optimization_barrier((half_share, matrix_new, normal_new))
    returned = exchange(half_share).astype(jnp.float32).reshape(experts, capacity, col_width)
    if every_row:
        routed = jnp.sum(returned * shares.T[:, :, None], axis=0)
    else:
        combine = jnp.sum(
            (table * shares.reshape(-1)[:, None]).reshape(
                seq_dev, top_count, experts * capacity
            ),
            axis=1,
        )
        routed = jnp.dot(
            combine, returned.reshape(experts * capacity, col_width), precision=lax.Precision.HIGHEST
        )
    mixed_out = (own_resid.astype(jnp.float32) + routed).astype(jnp.bfloat16)
    return (mixed_out, matrix_new, normal_new, stab_new)


def solution(mesh):
    placed = (
        P("ep", None),
        P(),
        P(),
        P("ep", "tp"),
        P("ep", "tp"),
        P("ep", "tp"),
        P("ep", "tp"),
        P(),
        P(),
        P(),
        P(),
        P("tp", None),
        P("ep", "tp", None, None),
        P("ep", "tp", None),
        P("ep", "tp"),
        P("ep", None),
        P("ep", None),
        P("ep", None, "tp"),
        P("ep", None, "tp"),
        P("ep", "tp", None),
    )
    return jax.shard_map(
        body,
        mesh=mesh,
        in_specs=placed,
        out_specs=(P("ep", "tp"), P("ep", "tp", None, None), P("ep", "tp", None), P("ep", "tp")),
        check_vma=False,
    )
```
